32 devices in a mesh: rep: 2 (over x), fs: 8 (over z, y), tp: 2 (over core).
Axes of the slice: x: 2, y: 2, z: 4, core: 2. Of those that a mesh axis runs over, the one named last changes fastest.
Arguments:
- gate_late: bfloat16 [6144, 4096], P(('rep', 'fs'), 'tp'), may hold values from -6 to 6
- up_late: bfloat16 [6144, 4096], P(('rep', 'fs'), 'tp'), may hold values from -6 to 6
- gate_early: bfloat16 [6144, 4096], P(('rep', 'fs'), 'tp'), may hold values from -6 to 6
- up_early: bfloat16 [6144, 4096], P(('rep', 'fs'), 'tp'), may hold values from -6 to 6
- cotangent: bfloat16 [6144, 2048], P(('rep', 'fs')), may hold values from -6 to 6
- w_down: bfloat16 [2048, 4096], P('fs', 'tp'), may hold values from -0.09375 to 0.09375
- grad_in: float32 [2048, 4096], P('fs', 'tp'), may hold values from -6 to 6
Outputs:
- late_out: bfloat16 [6144, 2048], P(('rep', 'fs'))
- gate_grad: bfloat16 [6144, 4096], P(('rep', 'fs'), 'tp')
- up_grad: bfloat16 [6144, 4096], P(('rep', 'fs'), 'tp')
- grad_out: float32 [2048, 4096], P('fs', 'tp')
The draws below stay inside these ranges and needn't reach their ends.
All inputs are finite; a program needn't handle non-finite values.
Results may differ from the reference program's by a relative error of at most 0.014.
Values may be sent and summed in bfloat16 or wider, within the bound.
A program may use at most 64 MiB of HBM per device.

```python
import jax
import jax.numpy as jnp
from jax import lax

D = 2048
FF = 4096
TOKENS = 6144
N_TP = 2


def spiked(result, own_key, source, target, blocks, factor):
    def block_of(position):
        return (jnp.arange(result.shape[position]) // (result.shape[position] // blocks)).reshape((-1,) + (1,) * (result.ndim - 1 - position))

    one_side = jax.random.permutation(own_key, blocks)[block_of(target)]
    other_side = (block_of(target) + blocks // 2) % blocks
    return jnp.where((block_of(source) == one_side) | (block_of(source) == other_side), factor * result, result)


def steps_of(own_key, extent, shards, smallest, largest):
    gain = 1.0
    for position, blocks in shards:
        steps = jax.random.uniform(jax.random.fold_in(jax.random.fold_in(own_key, 6), position), (blocks,), jnp.float32, smallest / len(shards), largest / len(shards))
        gain = gain * jnp.repeat(jnp.exp(steps), extent[position] // blocks).reshape((-1,) + (1,) * (len(extent) - 1 - position))
    return gain


def normal_values(key, dims, deviation, limit, pieces=(), kind=jnp.bfloat16):
    loudness = steps_of(key, dims, pieces, -0.22, 0.18) if pieces else 1.0
    result = jax.random.normal(key, dims, jnp.float32) * deviation * loudness
    return jnp.minimum(jnp.maximum(result, -limit), limit).astype(kind)


def gaussian_with(stream_key, shape, width, reach, cuts, heavy, kind=jnp.bfloat16):
    drawn = width * jax.random.normal(stream_key, shape, jnp.float32)
    if cuts:
        drawn = drawn * steps_of(stream_key, shape, cuts, -0.22, 0.18)
    return jnp.clip(spiked(drawn, jax.random.fold_in(stream_key, 3), *heavy), -reach, reach).astype(kind)


def setup_inputs(seed: int = 0) -> dict:
    splits = jax.random.split(jax.random.key(seed), 8)
    return {
        "gate_late": normal_values(splits[0], (TOKENS, FF), 1.0, 6.0, ((0, 16), (1, 2))),
        "up_late": normal_values(splits[1], (TOKENS, FF), 1.0, 6.0, ((0, 16), (1, 2))),
        "gate_early": normal_values(splits[2], (TOKENS, FF), 1.0, 6.0, ((0, 16), (1, 2))),
        "up_early": normal_values(splits[3], (TOKENS, FF), 1.0, 6.0, ((0, 16), (1, 2))),
        "cotangent": gaussian_with(splits[4], (TOKENS, D), 1.0, 6.0, ((0, 16),), (0, 1, 16, 2.0)),
        "w_down": normal_values(splits[5], (D, FF), FF ** -0.5, 0.09375, ((0, 8), (1, 2))),
        "grad_in": normal_values(splits[6], (D, FF), 1.0, 6.0, ((0, 8), (1, 2)), jnp.float32),
    }


def reference(gate_late, up_late, gate_early, up_early, cotangent, w_down, grad_in):
    gate_value = gate_late.astype(jnp.float32)
    hidden_late = (jax.nn.silu(gate_value) * up_late.astype(jnp.float32)).astype(jnp.bfloat16)
    block_width = FF // N_TP

    def add_block(block_index, running):
        offset = (block_index * block_width).astype(jnp.int32)
        hidden_block = lax.dynamic_slice_in_dim(hidden_late, offset, block_width, 1)
        weight_block = lax.dynamic_slice_in_dim(w_down, offset, block_width, 1)
        partial_value = lax.dot_general(hidden_block, weight_block, (((1,), (1,)), ((), ())), preferred_element_type=jnp.float32)
        rounded = lax.optimization_barrier(partial_value.astype(jnp.bfloat16))
        return running + rounded.astype(jnp.float32)
    summed = lax.fori_loop(0, N_TP, add_block, jnp.zeros((gate_late.shape[0], D), jnp.float32))
    late_out = summed.astype(jnp.bfloat16)
    gate_value = gate_early.astype(jnp.float32)
    sigmoid_early = jax.nn.sigmoid(gate_value)
    swish_early = gate_value * sigmoid_early
    up_value = up_early.astype(jnp.float32)
    hidden_early = (swish_early * up_value).astype(jnp.bfloat16)
    hidden_grad = jnp.dot(cotangent, w_down, preferred_element_type=jnp.float32)
    gate_grad = (hidden_grad * up_value * sigmoid_early * (1.0 + gate_value * (1.0 - sigmoid_early))).astype(jnp.bfloat16)
    up_grad = (hidden_grad * swish_early).astype(jnp.bfloat16)
    weight_grad = lax.dot_general(cotangent, hidden_early, (((0,), (0,)), ((), ())), preferred_element_type=jnp.float32)
    grad_out = grad_in + weight_grad * (1.0 / jnp.sqrt(jnp.float32(TOKENS)))
    return (late_out, gate_grad, up_grad, grad_out)
```

```python
import functools
import math

import jax
import jax.numpy as jnp
from jax import lax
from jax.experimental import pallas as pl
from jax.experimental.pallas import tpu as pltpu
from jax.sharding import PartitionSpec as P

MESH = pl.DeviceIdType.MESH
F32 = jnp.float32
BF16 = jnp.bfloat16
RIGHT, LEFT, ACROSS, OTHER = 0, 1, 2, 3
LAG = 3
USE_LAG = 6
SUM_LAG = 6
TILE = 16


def kernel(
    n, n_tp, chunks, scale,
    gl_h, ul_h, ge_h, ue_h, cot_h, w_h, gin_h,
    late, gg, ug, gout,
    gl, ul, ge, ue, cot, gin, wf, hl, he, he_out, hg, part, own, opp, ys, yr, zs, zr, yfs, yfr, xs, xr,
    ld, ag_s, ag_r, cx_s, cx_r, ct_s, ct_r, he_s, he_r, y_s, y_r, z_s, z_r, yf_s, yf_r, x_s, x_r, tp_s, tp_r,
):
    tokens, cols = gl.shape
    rows = wf.shape[1]
    quarter = rows // 4
    half = rows // 2
    nz = n // 2
    hq = cols // 2
    width = hq // chunks
    rep = lax.axis_index("rep")
    me = lax.axis_index("fs")
    tp = lax.axis_index("tp")
    z = lax.div(me, 2)
    y = lax.rem(me, 2)
    other = 1 - rep
    flat = len(cot.shape) == 2

    def cot_tokens(ref, start, size):
        return ref.at[pl.ds(start, size), :] if flat else ref.at[:, pl.ds(start, size), :]

    def loads(i):
        pairs = (
            (w_h, wf.at[me]), (cot_h, cot_tokens(cot, 0, tokens)), (ge_h, ge), (ue_h, ue),
            (gl_h, gl), (ul_h, ul), (gin_h, gin),
        )
        return pltpu.make_async_copy(pairs[i][0], pairs[i][1], ld.at[i])

    for i in range(7):
        loads(i).start()

    barrier = pltpu.get_barrier_semaphore()

    @pl.when(z < nz - 1)
    def _():
        pl.semaphore_signal(barrier, inc=1, device_id={"fs": me + 2}, device_id_type=MESH)

    @pl.when(z > 0)
    def _():
        pl.semaphore_signal(barrier, inc=1, device_id={"fs": me - 2}, device_id_type=MESH)

    pl.semaphore_signal(barrier, inc=1, device_id={"fs": 2 * z + 1 - y}, device_id_type=MESH)
    pl.semaphore_signal(barrier, inc=1, device_id={"rep": other}, device_id_type=MESH)
    for k in range(1, n_tp):
        pl.semaphore_signal(barrier, inc=1, device_id={"tp": lax.rem(tp + k, n_tp)}, device_id_type=MESH)
    inner = jnp.where((z > 0) & (z < nz - 1), 1, 0)
    pl.semaphore_wait(barrier, 2 + n_tp + inner)

    def target(way):
        if way == RIGHT:
            return {"fs": me + 2}
        if way == LEFT:
            return {"fs": me - 2}
        if way == ACROSS:
            return {"fs": 2 * z + 1 - y}
        return {"rep": other}

    def piece_rows(p):
        return pl.ds(pl.multiple_of((p + rep * (3 - 2 * p)) * quarter, 16), quarter)

    def piece(way, shard, p):
        spot = wf.at[shard, piece_rows(p), :]
        return pltpu.make_async_remote_copy(
            src_ref=spot, dst_ref=spot, send_sem=ag_s.at[way, shard, p],
            recv_sem=ag_r.at[shard, 3 if way == OTHER else p],
            device_id=target(way), device_id_type=MESH,
        )

    def piece_arrived(shard, p):
        spot = wf.at[shard, piece_rows(p), :]
        pltpu.make_async_remote_copy(
            src_ref=spot, dst_ref=spot, send_sem=ag_s.at[0, shard, 0], recv_sem=ag_r.at[shard, p],
            device_id=target(OTHER), device_id_type=MESH,
        ).wait_recv()

    loads(0).wait()
    for p in range(3):
        piece(ACROSS, me, (2, 0, 1)[p]).start()

        @pl.when(z < nz - 1)
        def _():
            piece(RIGHT, me, p).start()

        @pl.when(z > 0)
        def _():
            piece(LEFT, me, p).start()

    lot = tokens // n_tp

    def cot_cross():
        return pltpu.make_async_remote_copy(
            src_ref=cot_tokens(cot, pl.multiple_of(tp * lot, 16), lot),
            dst_ref=cot_tokens(cot, pl.multiple_of(tokens + tp * lot, 16), lot),
            send_sem=cx_s, recv_sem=cx_r, device_id={"rep": other}, device_id_type=MESH,
        )

    def cot_share(k, sender):
        spot = cot_tokens(cot, pl.multiple_of(tokens + sender * lot, 16), lot)
        return pltpu.make_async_remote_copy(
            src_ref=spot, dst_ref=spot, send_sem=ct_s.at[k], recv_sem=ct_r.at[k],
            device_id={"tp": lax.rem(tp + k, n_tp)}, device_id_type=MESH,
        )

    loads(1).wait()
    cot_cross().start()

    def columns(c):
        return pl.ds(pl.multiple_of(c * width, 128), width)

    def he_cross(c):
        return pltpu.make_async_remote_copy(
            src_ref=he_out.at[:, columns(c)], dst_ref=he.at[pl.ds(tokens, tokens), columns(c)],
            send_sem=he_s.at[c], recv_sem=he_r.at[c], device_id={"rep": other}, device_id_type=MESH,
        )

    def tile_at(i):
        return pl.ds(pl.multiple_of(i * TILE, TILE), TILE)

    def gated(gate_ref, up_ref, span, lanes):
        gate = gate_ref[span, lanes].astype(F32)
        return (gate * (1.0 / (1.0 + jnp.exp(-gate))) * up_ref[span, lanes].astype(F32)).astype(BF16)

    mine_lanes = pl.ds(pl.multiple_of(rep * hq, 128), hq)
    theirs_lanes = pl.ds(pl.multiple_of(other * hq, 128), hq)
    loads(2).wait()
    loads(3).wait()

    @pl.loop(0, tokens // TILE)
    def _(i):
        he_out[tile_at(i), :] = gated(ge, ue, tile_at(i), theirs_lanes)

    for c in range(chunks):
        he_cross(c).start()

    @pl.loop(0, tokens // TILE)
    def _(i):
        he[tile_at(i), :] = gated(ge, ue, tile_at(i), mine_lanes)

    beyond = 2 * z + 1 - y
    piece_arrived(beyond, 2)

    @pl.when(z < nz - 1)
    def _():
        piece(RIGHT, beyond, 2).start()

    @pl.when(z > 0)
    def _():
        piece(LEFT, beyond, 2).start()

    loads(4).wait()
    loads(5).wait()

    @pl.loop(0, tokens // TILE)
    def _(i):
        hl[tile_at(i), :] = gated(gl, ul, tile_at(i), slice(None))
        hg[tile_at(i), :] = jnp.zeros((TILE, cols), F32)

    def nearest(m):
        low = jnp.minimum(z, nz - 1 - z)
        paired = m <= 2 * low
        step = jnp.where(paired, lax.div(m + 1, 2), m - low)
        down = jnp.where(paired, lax.rem(m, 2) == 1, 2 * z > nz - 1)
        return jnp.where(down, z - step, z + step)

    def gather(k):
        hop = lax.div(k, 4) + 1
        p = lax.rem(k, 4)
        line = jnp.where(p == 3, 1 - y, y)
        q = jnp.where(p == 3, 2, p)
        for source, onward, way in ((z - hop, z + 1, RIGHT), (z + hop, z - 1, LEFT)):

            @pl.when((source >= 0) & (source < nz))
            def _():
                shard = 2 * source + line
                piece_arrived(shard, q)

                @pl.when((onward >= 0) & (onward < nz))
                def _():
                    piece(way, shard, q).start()

                @pl.when(p < 2)
                def _():
                    piece(ACROSS, shard, q).start()

                @pl.when(p == 0)
                def _():
                    piece(OTHER, shard, q).start()

    def gather_across(k):
        hop = lax.div(k, 4) + 1
        for source in (z - hop, z + hop):

            @pl.when((source >= 0) & (source < nz))
            def _():
                shard = 2 * source + 1 - y
                piece_arrived(shard, 0)
                piece(OTHER, shard, 0).start()

    def cot_block(first, size, shard):
        if flat:
            return cot[pl.ds(first, size), pl.ds(pl.multiple_of(shard * rows, rows), rows)]
        return cot[shard, pl.ds(first, size), :]

    def share(k, shard):
        return pltpu.make_async_remote_copy(
            src_ref=part.at[tp, shard], dst_ref=part.at[tp, shard],
            send_sem=tp_s.at[k, shard], recv_sem=tp_r.at[k, shard],
            device_id={"tp": lax.rem(tp + k, n_tp)}, device_id_type=MESH,
        )

    def share_arrived(k, shard):
        spot = part.at[lax.rem(tp + n_tp - k, n_tp), shard]
        pltpu.make_async_remote_copy(
            src_ref=spot, dst_ref=spot, send_sem=tp_s.at[k, shard], recv_sem=tp_r.at[k, shard],
            device_id={"tp": lax.rem(tp + k, n_tp)}, device_id_type=MESH,
        ).wait_recv()

    def use(i, carry):
        crossed = lax.rem(i, 2)
        line = jnp.where(crossed == 1, 1 - y, y)
        shard = 2 * nearest(lax.div(i, 2)) + line

        @pl.when(crossed == 1)
        def _():
            piece_arrived(shard, 1)

        @pl.when(i > 0)
        def _():
            piece_arrived(shard, 3)

        block = wf[shard]
        part[tp, shard] = lax.dot_general(
            hl[...], block, (((1,), (1,)), ((), ())), preferred_element_type=F32
        ).astype(BF16)
        for k in range(1, n_tp):
            share(k, shard).start()
        hg[...] += jnp.dot(cot_block(0, tokens, shard), block, preferred_element_type=F32)
        return carry

    def y_copy(c, to):
        return pltpu.make_async_remote_copy(
            src_ref=ys.at[c, to], dst_ref=yr.at[c, to], send_sem=y_s.at[c, to], recv_sem=y_r.at[c, to],
            device_id=target(ACROSS), device_id_type=MESH,
        )

    def z_copy(way, c, to):
        return pltpu.make_async_remote_copy(
            src_ref=zs.at[c, to], dst_ref=zr.at[way, c, to],
            send_sem=z_s.at[c, to], recv_sem=z_r.at[way, c, to],
            device_id=target(way), device_id_type=MESH,
        )

    def z_arrived(way, c, to):
        pltpu.make_async_remote_copy(
            src_ref=zs.at[c, to], dst_ref=zr.at[way, c, to],
            send_sem=z_s.at[c, to], recv_sem=z_r.at[way, c, to],
            device_id=target(OTHER), device_id_type=MESH,
        ).wait_recv()

    def yf_copy(c):
        return pltpu.make_async_remote_copy(
            src_ref=yfs.at[c], dst_ref=yfr.at[c], send_sem=yf_s.at[c], recv_sem=yf_r.at[c],
            device_id=target(ACROSS), device_id_type=MESH,
        )

    def x_copy(c):
        return pltpu.make_async_remote_copy(
            src_ref=xs.at[c], dst_ref=xr.at[c], send_sem=x_s.at[c], recv_sem=x_r.at[c],
            device_id={"rep": other}, device_id_type=MESH,
        )

    def contribute(c):
        he_cross(c).wait_recv()

        @pl.loop(0, nz)
        def _(m):
            to = nearest(nz - 1 - m)

            def term(line):
                return lax.dot_general(
                    cot_block(0, 2 * tokens, 2 * to + line), he[:, columns(c)],
                    (((0,), (0,)), ((), ())), preferred_element_type=F32,
                )

            value = term(1 - y)
            ys[c, to] = value[:half].astype(BF16)
            y_copy(c, to).start()
            opp[c, to] = value[half:]
            own[c, to] = term(y)

    top = pl.ds(0, half)
    mid = pl.ds(half, half)
    low = pl.ds(rows, half)

    def forward(s):
        for way, place in ((RIGHT, z), (LEFT, nz - 1 - z)):
            at = s + jnp.where(place == 0, 1, 0)
            safe = jnp.maximum(at, 0)
            c = lax.div(safe, nz - 1)
            j = lax.rem(safe, nz - 1) - place

            @pl.when((at >= 0) & (at < chunks * (nz - 1)) & (j >= 0))
            def _():
                to = nz - 1 - j if way == RIGHT else j
                y_copy(c, to).wait_recv()

                @pl.when(place == 0)
                def _():
                    zs[c, to, top, :] = (own[c, to, top, :] + yr[c, to].astype(F32)).astype(BF16)
                    zs[c, to, mid, :] = own[c, to, mid, :].astype(BF16)
                    zs[c, to, low, :] = opp[c, to].astype(BF16)

                @pl.when(place > 0)
                def _():
                    z_arrived(way, c, to)
                    before = zr.at[way, c, to]
                    zs[c, to, top, :] = (
                        own[c, to, top, :] + yr[c, to].astype(F32) + before[top, :].astype(F32)
                    ).astype(BF16)
                    zs[c, to, mid, :] = (own[c, to, mid, :] + before[mid, :].astype(F32)).astype(BF16)
                    zs[c, to, low, :] = (opp[c, to] + before[low, :].astype(F32)).astype(BF16)

                z_copy(way, c, to).start()

    def finish_line(c):
        y_copy(c, z).wait_recv()
        own[c, z, top, :] += yr[c, z].astype(F32)
        for way, there in ((RIGHT, z > 0), (LEFT, z < nz - 1)):

            @pl.when(there)
            def _():
                z_arrived(way, c, z)
                before = zr.at[way, c, z]
                opp[c, z] += before[low, :].astype(F32)
                own[c, z] += before[pl.ds(0, rows), :].astype(F32)

        yfs[c] = opp[c, z].astype(BF16)
        yf_copy(c).start()

    def finish_pair(c):
        yf_copy(c).wait_recv()
        own[c, z, mid, :] += yfr[c].astype(F32)
        xs[c] = own[c, z].astype(BF16)
        x_copy(c).start()
        lanes = pl.ds(pl.multiple_of(rep * hq + c * width, 128), width)
        gout[:, lanes] = gin[:, lanes] + own[c, z] * scale

    def finish_cross(c):
        x_copy(c).wait_recv()
        lanes = pl.ds(pl.multiple_of(other * hq + c * width, 128), width)
        gout[:, lanes] = gin[:, lanes] + xr[c].astype(F32) * scale

    def reduce_step(s):
        safe = jnp.maximum(s, 0)
        c = lax.div(safe, nz - 1)
        t = lax.rem(safe, nz - 1)
        ahead = jnp.where(s == -2, 0, c + 1)

        @pl.when(((s == -2) | ((s >= 0) & (t == 0))) & (ahead < chunks))
        def _():
            contribute(ahead)

        forward(s)
        done = c - 1

        @pl.when((t == 0) & (done >= 0) & (done < chunks))
        def _():
            finish_line(done)

        @pl.when((t == 1) & (done >= 0) & (done < chunks))
        def _():
            finish_pair(done)

        @pl.when((t == 2) & (done >= 0) & (done < chunks))
        def _():
            finish_cross(done)

    gather_ticks = 4 * (nz - 1)
    use_ticks = max(2 * n - 3, n + USE_LAG)
    sum_ticks = SUM_LAG + chunks * (nz - 1) + 2

    def used(k):
        return jnp.clip(jnp.minimum(lax.div(k + 2, 2), k - USE_LAG) + 1, 1, n)

    def tick(k, carry):
        @pl.when(k < gather_ticks)
        def _():
            gather(k)

        late_k = k - LAG

        @pl.when((late_k >= 0) & (late_k < gather_ticks) & (lax.rem(jnp.maximum(late_k, 0), 4) == 0))
        def _():
            gather_across(late_k)

        @pl.when(k == 1)
        def _():
            piece_arrived(beyond, 0)
            piece(OTHER, beyond, 0).start()

        @pl.when(k == SUM_LAG - 3)
        def _():
            cot_cross().wait_recv()
            for j in range(1, n_tp):
                cot_share(j, tp).start()

        @pl.when(k == SUM_LAG - 2)
        def _():
            for j in range(1, n_tp):
                cot_share(j, lax.rem(tp + n_tp - j, n_tp)).wait_recv()
            loads(6).wait()

        @pl.when((k >= SUM_LAG - 2) & (k < sum_ticks))
        def _():
            reduce_step(k - SUM_LAG)

        lax.fori_loop(jnp.where(k == 0, 0, used(k - 1)), used(k), use, 0)
        return carry

    lax.fori_loop(0, max(use_ticks, gather_ticks, sum_ticks), tick, 0)

    @pl.loop(0, tokens // TILE)
    def _(i):
        span = tile_at(i)
        gate = ge[span, :].astype(F32)
        sig = 1.0 / (1.0 + jnp.exp(-gate))
        grad = hg[span, :]
        ug[span, :] = (grad * (gate * sig)).astype(BF16)
        gg[span, :] = (
            grad * ue[span, :].astype(F32) * sig * (1.0 + gate * (1.0 - sig))
        ).astype(BF16)

    @pl.loop(0, n)
    def _(shard):
        for k in range(1, n_tp):
            share_arrived(k, shard)
        total = part[0, shard].astype(F32)
        for j in range(1, n_tp):
            total = total + part[j, shard].astype(F32)
        if flat:
            late[:, pl.ds(pl.multiple_of(shard * rows, rows), rows)] = total.astype(BF16)
        else:
            late[shard] = total.astype(BF16)

    reduce_step(jnp.int32(chunks * (nz - 1) + 2))

    cot_cross().wait_send()
    for k in range(1, n_tp):
        cot_share(k, tp).wait_send()
    for p in range(3):
        piece(ACROSS, me, p).wait_send()

    @pl.loop(0, nz)
    def _(at):
        same = 2 * at + y
        crossed = 2 * at + 1 - y

        @pl.when((at <= z) & (z < nz - 1))
        def _():
            for p in range(3):
                piece(RIGHT, same, p).wait_send()
            piece(RIGHT, crossed, 2).wait_send()

        @pl.when((at >= z) & (z > 0))
        def _():
            for p in range(3):
                piece(LEFT, same, p).wait_send()
            piece(LEFT, crossed, 2).wait_send()

        piece(OTHER, crossed, 0).wait_send()

        @pl.when(at != z)
        def _():
            piece(OTHER, same, 0).wait_send()
            for p in range(2):
                piece(ACROSS, same, p).wait_send()

        for k in range(1, n_tp):
            share(k, same).wait_send()
            share(k, crossed).wait_send()

        @pl.loop(0, chunks)
        def _(c):
            y_copy(c, at).wait_send()

            @pl.when(at > z)
            def _():
                z_copy(RIGHT, c, at).wait_send()

            @pl.when(at < z)
            def _():
                z_copy(LEFT, c, at).wait_send()

    @pl.loop(0, chunks)
    def _(c):
        he_cross(c).wait_send()
        yf_copy(c).wait_send()
        x_copy(c).wait_send()


def solution(mesh):
    n, n_tp, n_rep = mesh.shape["fs"], mesh.shape["tp"], mesh.shape["rep"]
    assert n_rep == 2 and n % 2 == 0 and n >= 8

    def per_device(gl, ul, ge, ue, cotangent, w, gin):
        tokens, cols = gl.shape
        rows, width = w.shape[0], cotangent.shape[1]
        assert rows % 64 == 0 and cols % 256 == 0
        nz, hq, half = n // 2, cols // 2, rows // 2
        chunks = 2
        scale = 1.0 / math.sqrt(tokens * n_rep * n)
        whole_lanes = rows % 128 == 0
        cot = cotangent
        if not whole_lanes:
            cot = cotangent.reshape(tokens, n, rows).transpose(1, 0, 2)
        cot_both = (2 * tokens, width) if whole_lanes else (n, 2 * tokens, rows)
        vmem = pl.BlockSpec(memory_space=pltpu.VMEM)
        dma = pltpu.SemaphoreType.DMA
        part = hq // chunks
        late, gg, ug, gout = pl.pallas_call(
            functools.partial(kernel, n, n_tp, chunks, scale),
            out_shape=(
                jax.ShapeDtypeStruct(cot.shape, BF16),
                jax.ShapeDtypeStruct((tokens, cols), BF16),
                jax.ShapeDtypeStruct((tokens, cols), BF16),
                jax.ShapeDtypeStruct((rows, cols), F32),
            ),
            in_specs=[pl.BlockSpec(memory_space=pl.ANY)] * 7,
            out_specs=(vmem,) * 4,
            scratch_shapes=[
                pltpu.VMEM((tokens, cols), BF16),
                pltpu.VMEM((tokens, cols), BF16),
                pltpu.VMEM((tokens, cols), BF16),
                pltpu.VMEM((tokens, cols), BF16),
                pltpu.VMEM(cot_both, BF16),
                pltpu.VMEM((rows, cols), F32),
                pltpu.VMEM((n, rows, cols), BF16),
                pltpu.VMEM((tokens, cols), BF16),
                pltpu.VMEM((2 * tokens, hq), BF16),
                pltpu.VMEM((tokens, hq), BF16),
                pltpu.VMEM((tokens, cols), F32),
                pltpu.VMEM((n_tp, n, tokens, rows), BF16),
                pltpu.VMEM((chunks, nz, rows, part), F32),
                pltpu.VMEM((chunks, nz, half, part), F32),
                pltpu.VMEM((chunks, nz, half, part), BF16),
                pltpu.VMEM((chunks, nz, half, part), BF16),
                pltpu.VMEM((chunks, nz, rows + half, part), BF16),
                pltpu.VMEM((2, chunks, nz, rows + half, part), BF16),
                pltpu.VMEM((chunks, half, part), BF16),
                pltpu.VMEM((chunks, half, part), BF16),
                pltpu.VMEM((chunks, rows, part), BF16),
                pltpu.VMEM((chunks, rows, part), BF16),
                dma((7,)),
                dma((4, n, 3)),
                dma((n, 4)),
                dma,
                dma,
                dma((n_tp,)),
                dma((n_tp,)),
                dma((chunks,)),
                dma((chunks,)),
                dma((chunks, nz)),
                dma((chunks, nz)),
                dma((chunks, nz)),
                dma((2, chunks, nz)),
                dma((chunks,)),
                dma((chunks,)),
                dma((chunks,)),
                dma((chunks,)),
                dma((n_tp, n)),
                dma((n_tp, n)),
            ],
            compiler_params=pltpu.CompilerParams(
                collective_id=0, has_side_effects=True, vmem_limit_bytes=67043328
            ),
        )(gl, ul, ge, ue, cot, w, gin)
        if not whole_lanes:
            late = late.transpose(1, 0, 2).reshape(tokens, width)
        return late, gg, ug, gout

    placed = (
        P(("rep", "fs"), "tp"),
        P(("rep", "fs"), "tp"),
        P(("rep", "fs"), "tp"),
        P(("rep", "fs"), "tp"),
        P(("rep", "fs"), None),
        P("fs", "tp"),
        P("fs", "tp"),
    )
    return jax.shard_map(
        per_device,
        mesh=mesh,
        in_specs=placed,
        out_specs=(
            P(("rep", "fs"), None),
            P(("rep", "fs"), "tp"),
            P(("rep", "fs"), "tp"),
            P("fs", "tp"),
        ),
        check_vma=False,
    )
```

```python
import functools
import math

import jax
import jax.numpy as jnp
from jax import lax
from jax.experimental import pallas as pl
from jax.experimental.pallas import tpu as pltpu
from jax.sharding import PartitionSpec as P

MESH = pl.DeviceIdType.MESH
F32 = jnp.float32
BF16 = jnp.bfloat16
RIGHT, LEFT, ACROSS, OTHER = 0, 1, 2, 3
LIMIT = 56 << 20
LAG = 3
USE_LAG = 6
START = 3
RATE = 1
CHUNKS = 2
LEAD = 1
AHEAD = 2
SETTLE = 0
DEFER = 4
TILE = 16


def kernel(
    n, n_tp, chunks, scale,
    gl_h, ul_h, ge_h, ue_h, cot_h, w_h, gin_h,
    late, gg, ug, gout,
    gl, ul, ge, ue, cot, gin, wf, hl, he, he_out, hg, part, own, opp, ys, yr, zs, zr, yfs, yfr, xs, xr,
    ld, ag_s, ag_r, cx_s, cx_r, ct_s, ct_r, he_s, he_r, y_s, y_r, z_s, z_r, yf_s, yf_r, x_s, x_r, tp_s, tp_r,
):
    tokens, cols = gl.shape
    rows = wf.shape[1]
    quarter = rows // 4
    half = rows // 2
    nz = n // 2
    hq = cols // 2
    width = hq // chunks
    rep = lax.axis_index("rep")
    me = lax.axis_index("fs")
    tp = lax.axis_index("tp")
    z = lax.div(me, 2)
    y = lax.rem(me, 2)
    other = 1 - rep
    flat = len(cot.shape) == 2

    def cot_tokens(ref, start, size):
        return ref.at[pl.ds(start, size), :] if flat else ref.at[:, pl.ds(start, size), :]

    def loads(i):
        pairs = (
            (w_h, wf.at[me]), (cot_h, cot_tokens(cot, 0, tokens)), (ge_h, ge), (ue_h, ue),
            (gl_h, gl), (ul_h, ul), (gin_h, gin),
        )
        return pltpu.make_async_copy(pairs[i][0], pairs[i][1], ld.at[i])

    for i in range(7):
        loads(i).start()

    barrier = pltpu.get_barrier_semaphore()

    @pl.when(z < nz - 1)
    def _():
        pl.semaphore_signal(barrier, inc=1, device_id={"fs": me + 2}, device_id_type=MESH)

    @pl.when(z > 0)
    def _():
        pl.semaphore_signal(barrier, inc=1, device_id={"fs": me - 2}, device_id_type=MESH)

    pl.semaphore_signal(barrier, inc=1, device_id={"fs": 2 * z + 1 - y}, device_id_type=MESH)
    pl.semaphore_signal(barrier, inc=1, device_id={"rep": other}, device_id_type=MESH)
    for k in range(1, n_tp):
        pl.semaphore_signal(barrier, inc=1, device_id={"tp": lax.rem(tp + k, n_tp)}, device_id_type=MESH)
    inner = jnp.where((z > 0) & (z < nz - 1), 1, 0)
    pl.semaphore_wait(barrier, 2 + n_tp + inner)

    def target(way):
        if way == RIGHT:
            return {"fs": me + 2}
        if way == LEFT:
            return {"fs": me - 2}
        if way == ACROSS:
            return {"fs": 2 * z + 1 - y}
        return {"rep": other}

    def piece_rows(p):
        return pl.ds(pl.multiple_of((p + rep * (3 - 2 * p)) * quarter, 16), quarter)

    def piece(way, shard, p):
        spot = wf.at[shard, piece_rows(p), :]
        return pltpu.make_async_remote_copy(
            src_ref=spot, dst_ref=spot, send_sem=ag_s.at[way, shard, p],
            recv_sem=ag_r.at[shard, 3 if way == OTHER else p],
            device_id=target(way), device_id_type=MESH,
        )

    def piece_arrived(shard, p):
        spot = wf.at[shard, piece_rows(p), :]
        pltpu.make_async_remote_copy(
            src_ref=spot, dst_ref=spot, send_sem=ag_s.at[0, shard, 0], recv_sem=ag_r.at[shard, p],
            device_id=target(OTHER), device_id_type=MESH,
        ).wait_recv()

    loads(0).wait()
    for p in range(3):
        piece(ACROSS, me, (2, 0, 1)[p]).start()

        @pl.when(z < nz - 1)
        def _():
            piece(RIGHT, me, p).start()

        @pl.when(z > 0)
        def _():
            piece(LEFT, me, p).start()

    lot = tokens // n_tp

    def cot_cross():
        return pltpu.make_async_remote_copy(
            src_ref=cot_tokens(cot, pl.multiple_of(tp * lot, 16), lot),
            dst_ref=cot_tokens(cot, pl.multiple_of(tokens + tp * lot, 16), lot),
            send_sem=cx_s, recv_sem=cx_r, device_id={"rep": other}, device_id_type=MESH,
        )

    def cot_share(k, sender):
        spot = cot_tokens(cot, pl.multiple_of(tokens + sender * lot, 16), lot)
        return pltpu.make_async_remote_copy(
            src_ref=spot, dst_ref=spot, send_sem=ct_s.at[k], recv_sem=ct_r.at[k],
            device_id={"tp": lax.rem(tp + k, n_tp)}, device_id_type=MESH,
        )

    loads(1).wait()
    cot_cross().start()

    def columns(c):
        return pl.ds(pl.multiple_of(c * width, 128), width)

    def he_cross(c):
        return pltpu.make_async_remote_copy(
            src_ref=he_out.at[:, columns(c)], dst_ref=he.at[pl.ds(tokens, tokens), columns(c)],
            send_sem=he_s.at[c], recv_sem=he_r.at[c], device_id={"rep": other}, device_id_type=MESH,
        )

    def tile_at(i):
        return pl.ds(pl.multiple_of(i * TILE, TILE), TILE)

    def gated(gate_ref, up_ref, span, lanes):
        gate = gate_ref[span, lanes].astype(F32)
        return (gate * (1.0 / (1.0 + jnp.exp(-gate))) * up_ref[span, lanes].astype(F32)).astype(BF16)

    mine_lanes = pl.ds(pl.multiple_of(rep * hq, 128), hq)
    theirs_lanes = pl.ds(pl.multiple_of(other * hq, 128), hq)
    loads(2).wait()
    loads(3).wait()

    @pl.loop(0, tokens // TILE)
    def _(i):
        he_out[tile_at(i), :] = gated(ge, ue, tile_at(i), theirs_lanes)

    for c in range(chunks):
        he_cross(c).start()

    @pl.loop(0, tokens // TILE)
    def _(i):
        he[tile_at(i), :] = gated(ge, ue, tile_at(i), mine_lanes)

    beyond = 2 * z + 1 - y
    piece_arrived(beyond, 2)

    @pl.when(z < nz - 1)
    def _():
        piece(RIGHT, beyond, 2).start()

    @pl.when(z > 0)
    def _():
        piece(LEFT, beyond, 2).start()

    loads(4).wait()
    loads(5).wait()

    @pl.loop(0, tokens // TILE)
    def _(i):
        hl[tile_at(i), :] = gated(gl, ul, tile_at(i), slice(None))
        hg[tile_at(i), :] = jnp.zeros((TILE, cols), F32)

    def nearest(m):
        low = jnp.minimum(z, nz - 1 - z)
        paired = m <= 2 * low
        step = jnp.where(paired, lax.div(m + 1, 2), m - low)
        down = jnp.where(paired, lax.rem(m, 2) == 1, 2 * z > nz - 1)
        return jnp.where(down, z - step, z + step)

    def gather(k):
        hop = lax.div(k, 4) + 1
        p = lax.rem(k, 4)
        line = jnp.where(p == 3, 1 - y, y)
        q = jnp.where(p == 3, 2, p)
        for source, onward, way in ((z - hop, z + 1, RIGHT), (z + hop, z - 1, LEFT)):

            @pl.when((source >= 0) & (source < nz))
            def _():
                shard = 2 * source + line
                piece_arrived(shard, q)

                @pl.when((onward >= 0) & (onward < nz))
                def _():
                    piece(way, shard, q).start()

                @pl.when((p == 0) | ((p == 1) & (hop > 1)))
                def _():
                    piece(ACROSS, shard, q).start()

                @pl.when(p == 0)
                def _():
                    piece(OTHER, shard, q).start()

    def deferred():
        for source in (z - 1, z + 1):

            @pl.when((source >= 0) & (source < nz))
            def _():
                piece(ACROSS, 2 * source + y, 1).start()

    def gather_across(k):
        hop = lax.div(k, 4) + 1
        for source in (z - hop, z + hop):

            @pl.when((source >= 0) & (source < nz))
            def _():
                shard = 2 * source + 1 - y
                piece_arrived(shard, 0)
                piece(OTHER, shard, 0).start()

    def cot_block(first, size, shard):
        if flat:
            return cot[pl.ds(first, size), pl.ds(pl.multiple_of(shard * rows, rows), rows)]
        return cot[shard, pl.ds(first, size), :]

    def share(k, shard):
        return pltpu.make_async_remote_copy(
            src_ref=part.at[tp, shard], dst_ref=part.at[tp, shard],
            send_sem=tp_s.at[k, shard], recv_sem=tp_r.at[k, shard],
            device_id={"tp": lax.rem(tp + k, n_tp)}, device_id_type=MESH,
        )

    def share_arrived(k, shard):
        spot = part.at[lax.rem(tp + n_tp - k, n_tp), shard]
        pltpu.make_async_remote_copy(
            src_ref=spot, dst_ref=spot, send_sem=tp_s.at[k, shard], recv_sem=tp_r.at[k, shard],
            device_id={"tp": lax.rem(tp + k, n_tp)}, device_id_type=MESH,
        ).wait_recv()

    def use(i, carry):
        crossed = lax.rem(i, 2)
        line = jnp.where(crossed == 1, 1 - y, y)
        shard = 2 * nearest(lax.div(i, 2)) + line

        @pl.when(crossed == 1)
        def _():
            piece_arrived(shard, 1)

        @pl.when(i > 0)
        def _():
            piece_arrived(shard, 3)

        block = wf[shard]
        part[tp, shard] = lax.dot_general(
            hl[...], block, (((1,), (1,)), ((), ())), preferred_element_type=F32
        ).astype(BF16)
        for k in range(1, n_tp):
            share(k, shard).start()
        hg[...] += jnp.dot(cot_block(0, tokens, shard), block, preferred_element_type=F32)
        return carry

    def y_copy(c, to):
        return pltpu.make_async_remote_copy(
            src_ref=ys.at[c, to], dst_ref=yr.at[c, to], send_sem=y_s.at[c, to], recv_sem=y_r.at[c, to],
            device_id=target(ACROSS), device_id_type=MESH,
        )

    bulk = pl.ds(0, rows)
    rest = pl.ds(rows, half)

    def z_copy(way, c, to, stage, towards=None):
        span = (bulk, rest)[stage]
        return pltpu.make_async_remote_copy(
            src_ref=zs.at[c, to, span, :], dst_ref=zr.at[way, c, to, span, :],
            send_sem=z_s.at[stage, c, to], recv_sem=z_r.at[2 * way + stage, c, to],
            device_id=target(way if towards is None else towards), device_id_type=MESH,
        )

    def z_arrived(way, c, to, stage):
        z_copy(way, c, to, stage, OTHER).wait_recv()

    def yf_copy(c):
        return pltpu.make_async_remote_copy(
            src_ref=yfs.at[c], dst_ref=yfr.at[c], send_sem=yf_s.at[c], recv_sem=yf_r.at[c],
            device_id=target(ACROSS), device_id_type=MESH,
        )

    def x_copy(c, stage):
        return pltpu.make_async_remote_copy(
            src_ref=xs.at[c, stage], dst_ref=xr.at[c, stage],
            send_sem=x_s.at[stage, c], recv_sem=x_r.at[stage, c],
            device_id={"rep": other}, device_id_type=MESH,
        )

    def contribute(c):
        he_cross(c).wait_recv()

        @pl.loop(0, nz)
        def _(m):
            to = nearest(nz - 1 - m)

            def term(line):
                return lax.dot_general(
                    cot_block(0, 2 * tokens, 2 * to + line), he[:, columns(c)],
                    (((0,), (0,)), ((), ())), preferred_element_type=F32,
                )

            value = term(1 - y)
            ys[c, to] = value[:half].astype(BF16)
            y_copy(c, to).start()
            opp[c, to] = value[half:]
            own[c, to] = term(y)

    first, second = pl.ds(0, half), pl.ds(half, half)

    def forward(s):
        for way, place in ((RIGHT, z), (LEFT, nz - 1 - z)):
            at = s + jnp.where(place == 0, LEAD, 0)
            safe = jnp.maximum(at, 0)
            c = lax.div(safe, nz - 1)
            j = lax.rem(safe, nz - 1) - place

            @pl.when((at >= 0) & (at < chunks * (nz - 1)) & (j >= 0))
            def _():
                to = nz - 1 - j if way == RIGHT else j

                @pl.when(place == 0)
                def _():
                    zs[c, to, first, :] = own[c, to, second, :].astype(BF16)
                    zs[c, to, second, :] = opp[c, to].astype(BF16)

                @pl.when(place > 0)
                def _():
                    z_arrived(way, c, to, 0)
                    before = zr.at[way, c, to]
                    zs[c, to, first, :] = (own[c, to, second, :] + before[first, :].astype(F32)).astype(BF16)
                    zs[c, to, second, :] = (opp[c, to] + before[second, :].astype(F32)).astype(BF16)

                z_copy(way, c, to, 0).start()
                y_copy(c, to).wait_recv()

                @pl.when(place == 0)
                def _():
                    zs[c, to, rest, :] = (own[c, to, first, :] + yr[c, to].astype(F32)).astype(BF16)

                @pl.when(place > 0)
                def _():
                    z_arrived(way, c, to, 1)
                    zs[c, to, rest, :] = (
                        own[c, to, first, :] + yr[c, to].astype(F32) + zr[way, c, to, rest, :].astype(F32)
                    ).astype(BF16)

                z_copy(way, c, to, 1).start()

    sides = ((RIGHT, z > 0), (LEFT, z < nz - 1))

    def finish_line(c):
        for way, there in sides:

            @pl.when(there)
            def _():
                z_arrived(way, c, z, 0)
                before = zr.at[way, c, z]
                opp[c, z] += before[second, :].astype(F32)
                own[c, z, second, :] += before[first, :].astype(F32)

        yfs[c] = opp[c, z].astype(BF16)
        yf_copy(c).start()
        y_copy(c, z).wait_recv()
        own[c, z, first, :] += yr[c, z].astype(F32)
        for way, there in sides:

            @pl.when(there)
            def _():
                z_arrived(way, c, z, 1)
                own[c, z, first, :] += zr[way, c, z, rest, :].astype(F32)

        xs[c, 0] = own[c, z, first, :].astype(BF16)
        x_copy(c, 0).start()

    def finish_pair(c):
        yf_copy(c).wait_recv()
        own[c, z, second, :] += yfr[c].astype(F32)
        xs[c, 1] = own[c, z, second, :].astype(BF16)
        x_copy(c, 1).start()
        lanes = pl.ds(pl.multiple_of(rep * hq + c * width, 128), width)
        gout[:, lanes] = gin[:, lanes] + own[c, z] * scale

    def finish_cross(c):
        lanes = pl.ds(pl.multiple_of(other * hq + c * width, 128), width)
        for stage, span in ((0, first), (1, second)):
            x_copy(c, stage).wait_recv()
            gout[span, lanes] = gin[span, lanes] + xr[c, stage].astype(F32) * scale

    def reduce_step(s):
        def when_due(offset, ready, act):
            at = s - offset
            safe = jnp.maximum(at, 0)
            c = lax.div(safe, nz - 1) + ready

            @pl.when((at >= 0) & (lax.rem(safe, nz - 1) == 0) & (c >= 0) & (c < chunks))
            def _():
                act(c)

        when_due(-LEAD - AHEAD, 0, contribute)
        forward(s)
        when_due(SETTLE, -1, finish_line)
        when_due(SETTLE + 1, -1, finish_pair)
        when_due(SETTLE + 2, -1, finish_cross)

    gather_ticks = 4 * (nz - 1)
    use_ticks = max(2 * n - 3, n + USE_LAG)
    sum_steps = chunks * (nz - 1) + LEAD + AHEAD + SETTLE + 2
    sum_ticks = START + -(-sum_steps // RATE)

    def used(k):
        return jnp.clip(jnp.minimum(lax.div(k + 2, 2), k - USE_LAG) + 1, 1, n)

    def tick(k, carry):
        @pl.when(k < gather_ticks)
        def _():
            gather(k)

        late_k = k - LAG

        @pl.when((late_k >= 0) & (late_k < gather_ticks) & (lax.rem(jnp.maximum(late_k, 0), 4) == 0))
        def _():
            gather_across(late_k)

        @pl.when(k == 1)
        def _():
            piece_arrived(beyond, 0)
            piece(OTHER, beyond, 0).start()

        @pl.when(k == START - 1)
        def _():
            cot_cross().wait_recv()
            for j in range(1, n_tp):
                cot_share(j, tp).start()

        @pl.when(k == START)
        def _():
            for j in range(1, n_tp):
                cot_share(j, lax.rem(tp + n_tp - j, n_tp)).wait_recv()
            loads(6).wait()

        for r in range(RATE):
            step = (k - START) * RATE + r

            @pl.when((step >= 0) & (step < sum_steps))
            def _():
                reduce_step(step - LEAD - AHEAD)

        @pl.when(k == DEFER)
        def _():
            deferred()

        lax.fori_loop(jnp.where(k == 0, 0, used(k - 1)), used(k), use, 0)
        return carry

    lax.fori_loop(0, max(use_ticks, gather_ticks, sum_ticks), tick, 0)

    @pl.loop(0, tokens // TILE)
    def _(i):
        span = tile_at(i)
        gate = ge[span, :].astype(F32)
        sig = 1.0 / (1.0 + jnp.exp(-gate))
        grad = hg[span, :]
        ug[span, :] = (grad * (gate * sig)).astype(BF16)
        gg[span, :] = (
            grad * ue[span, :].astype(F32) * sig * (1.0 + gate * (1.0 - sig))
        ).astype(BF16)

    @pl.loop(0, n)
    def _(shard):
        for k in range(1, n_tp):
            share_arrived(k, shard)
        total = part[0, shard].astype(F32)
        for j in range(1, n_tp):
            total = total + part[j, shard].astype(F32)
        if flat:
            late[:, pl.ds(pl.multiple_of(shard * rows, rows), rows)] = total.astype(BF16)
        else:
            late[shard] = total.astype(BF16)

    reduce_step(jnp.int32(chunks * (nz - 1) + SETTLE + 2))

    cot_cross().wait_send()
    for k in range(1, n_tp):
        cot_share(k, tp).wait_send()
    for p in range(3):
        piece(ACROSS, me, p).wait_send()

    @pl.loop(0, nz)
    def _(at):
        same = 2 * at + y
        crossed = 2 * at + 1 - y

        @pl.when((at <= z) & (z < nz - 1))
        def _():
            for p in range(3):
                piece(RIGHT, same, p).wait_send()
            piece(RIGHT, crossed, 2).wait_send()

        @pl.when((at >= z) & (z > 0))
        def _():
            for p in range(3):
                piece(LEFT, same, p).wait_send()
            piece(LEFT, crossed, 2).wait_send()

        piece(OTHER, crossed, 0).wait_send()

        @pl.when(at != z)
        def _():
            piece(OTHER, same, 0).wait_send()
            for p in range(2):
                piece(ACROSS, same, p).wait_send()

        for k in range(1, n_tp):
            share(k, same).wait_send()
            share(k, crossed).wait_send()

        @pl.loop(0, chunks)
        def _(c):
            y_copy(c, at).wait_send()

            @pl.when(at > z)
            def _():
                z_copy(RIGHT, c, at, 0).wait_send()
                z_copy(RIGHT, c, at, 1).wait_send()

            @pl.when(at < z)
            def _():
                z_copy(LEFT, c, at, 0).wait_send()
                z_copy(LEFT, c, at, 1).wait_send()

    @pl.loop(0, chunks)
    def _(c):
        he_cross(c).wait_send()
        yf_copy(c).wait_send()
        x_copy(c, 0).wait_send()
        x_copy(c, 1).wait_send()


def deliver(*refs):
    count = 4
    sems = refs[-1]
    copies = [
        pltpu.make_async_copy(refs[i], refs[count + i], sems.at[i]) for i in range(count)
    ]
    for copy in copies:
        copy.start()
    for copy in copies:
        copy.wait()


def solution(mesh):
    n, n_tp, n_rep = mesh.shape["fs"], mesh.shape["tp"], mesh.shape["rep"]
    assert n_rep == 2 and n % 2 == 0 and n >= 8

    def per_device(gl, ul, ge, ue, cotangent, w, gin):
        tokens, cols = gl.shape
        rows, width = w.shape[0], cotangent.shape[1]
        assert rows % 64 == 0 and cols % 256 == 0
        nz, hq, half = n // 2, cols // 2, rows // 2
        chunks = min(CHUNKS, hq // 128)
        scale = 1.0 / math.sqrt(tokens * n_rep * n)
        whole_lanes = rows % 128 == 0
        cot = cotangent
        if not whole_lanes:
            cot = cotangent.reshape(tokens, n, rows).transpose(1, 0, 2)
        cot_both = (2 * tokens, width) if whole_lanes else (n, 2 * tokens, rows)
        vmem = pl.BlockSpec(memory_space=pltpu.VMEM)
        dma = pltpu.SemaphoreType.DMA
        part = hq // chunks
        late, gg, ug, gout = pl.pallas_call(
            functools.partial(kernel, n, n_tp, chunks, scale),
            out_shape=(
                pltpu.VMEM(cot.shape, BF16),
                pltpu.VMEM((tokens, cols), BF16),
                pltpu.VMEM((tokens, cols), BF16),
                pltpu.VMEM((rows, cols), F32),
            ),
            in_specs=[pl.BlockSpec(memory_space=pl.ANY)] * 7,
            out_specs=(vmem,) * 4,
            scratch_shapes=[
                pltpu.VMEM((tokens, cols), BF16),
                pltpu.VMEM((tokens, cols), BF16),
                pltpu.VMEM((tokens, cols), BF16),
                pltpu.VMEM((tokens, cols), BF16),
                pltpu.VMEM(cot_both, BF16),
                pltpu.VMEM((rows, cols), F32),
                pltpu.VMEM((n, rows, cols), BF16),
                pltpu.VMEM((tokens, cols), BF16),
                pltpu.VMEM((2 * tokens, hq), BF16),
                pltpu.VMEM((tokens, hq), BF16),
                pltpu.VMEM((tokens, cols), F32),
                pltpu.VMEM((n_tp, n, tokens, rows), BF16),
                pltpu.VMEM((chunks, nz, rows, part), F32),
                pltpu.VMEM((chunks, nz, half, part), F32),
                pltpu.VMEM((chunks, nz, half, part), BF16),
                pltpu.VMEM((chunks, nz, half, part), BF16),
                pltpu.VMEM((chunks, nz, rows + half, part), BF16),
                pltpu.VMEM((2, chunks, nz, rows + half, part), BF16),
                pltpu.VMEM((chunks, half, part), BF16),
                pltpu.VMEM((chunks, half, part), BF16),
                pltpu.VMEM((chunks, 2, half, part), BF16),
                pltpu.VMEM((chunks, 2, half, part), BF16),
                dma((7,)),
                dma((4, n, 3)),
                dma((n, 4)),
                dma,
                dma,
                dma((n_tp,)),
                dma((n_tp,)),
                dma((chunks,)),
                dma((chunks,)),
                dma((chunks, nz)),
                dma((chunks, nz)),
                dma((2, chunks, nz)),
                dma((4, chunks, nz)),
                dma((chunks,)),
                dma((chunks,)),
                dma((2, chunks)),
                dma((2, chunks)),
                dma((n_tp, n)),
                dma((n_tp, n)),
            ],
            compiler_params=pltpu.CompilerParams(
                collective_id=0, has_side_effects=True, vmem_limit_bytes=LIMIT
            ),
        )(gl, ul, ge, ue, cot, w, gin)
        late, gg, ug, gout = pl.pallas_call(
            deliver,
            out_shape=tuple(jax.ShapeDtypeStruct(a.shape, a.dtype) for a in (late, gg, ug, gout)),
            in_specs=[pl.BlockSpec(memory_space=pl.ANY)] * 4,
            out_specs=(pl.BlockSpec(memory_space=pl.ANY),) * 4,
            scratch_shapes=[dma((4,))],
            compiler_params=pltpu.CompilerParams(vmem_limit_bytes=1 << 20),
        )(late, gg, ug, gout)
        if not whole_lanes:
            late = late.transpose(1, 0, 2).reshape(tokens, width)
        return late, gg, ug, gout

    placed = (
        P(("rep", "fs"), "tp"),
        P(("rep", "fs"), "tp"),
        P(("rep", "fs"), "tp"),
        P(("rep", "fs"), "tp"),
        P(("rep", "fs"), None),
        P("fs", "tp"),
        P("fs", "tp"),
    )
    return jax.shard_map(
        per_device,
        mesh=mesh,
        in_specs=placed,
        out_specs=(
            P(("rep", "fs"), None),
            P(("rep", "fs"), "tp"),
            P(("rep", "fs"), "tp"),
            P("fs", "tp"),
        ),
        check_vma=False,
    )
```

```python
import functools
import math

import jax
import jax.numpy as jnp
from jax import lax
from jax.experimental import pallas as pl
from jax.experimental.pallas import tpu as pltpu
from jax.sharding import PartitionSpec as P

MESH = pl.DeviceIdType.MESH
F32 = jnp.float32
BF16 = jnp.bfloat16
RIGHT, LEFT, ACROSS, OTHER = 0, 1, 2, 3
LIMIT = 56 << 20
CHUNKS = 2
LEAD = 2
AHEAD = (1, 3)
SETTLE = (1, 1)
START = (2, 1)
LAG = (2, 5)
USE_LAG = (5, 7)
Y0 = 0
Y1 = 1
Y1H = 1
F1 = (1, 0)
RSFIRST = 1
YI = 1
HOLD = 1
FP = (2, 2)
FC = (2, 2)
P1 = 5
H0 = 7
TILE = 16


def kernel(
    n, n_tp, chunks, scale,
    gl_h, ul_h, ge_h, ue_h, cot_h, w_h, gin_h,
    late, gg, ug, gout,
    gl, ul, ge, ue, cot, gin, wf, hl, he, he_out, hg, part, own, opp, ys, yr, zs, zr, yfs, yfr, xs, xr,
    ld, ag_s, ag_r, cx_s, cx_r, ct_s, ct_r, he_s, he_r, y_s, y_r, z_s, z_r, yf_s, yf_r, x_s, x_r, tp_s, tp_r,
):
    tokens, cols = gl.shape
    rows = wf.shape[1]
    quarter = rows // 4
    third = max(rows * P1 // 256, 1) * 16
    head = max(rows * H0 // 256, 1) * 16
    tail = rows - head
    nz = n // 2
    hq = cols // 2
    width = hq // chunks
    rep = lax.axis_index("rep")
    me = lax.axis_index("fs")
    tp = lax.axis_index("tp")
    z = lax.div(me, 2)
    y = lax.rem(me, 2)
    other = 1 - rep
    flat = len(cot.shape) == 2
    end = (z == 0) | (z == nz - 1)

    def pick(pair):
        return pair[0] if pair[0] == pair[1] else jnp.where(end, pair[0], pair[1])

    lead, ahead, settle = LEAD, pick(AHEAD), pick(SETTLE)
    begin, lag, use_lag, split = pick(START), pick(LAG), pick(USE_LAG), pick(F1)
    pair_due = settle + pick(FP)
    cross_due = pair_due + pick(FC)

    def cot_tokens(ref, start, size):
        return ref.at[pl.ds(start, size), :] if flat else ref.at[:, pl.ds(start, size), :]

    def loads(i):
        pairs = (
            (w_h, wf.at[me]), (cot_h, cot_tokens(cot, 0, tokens)), (ge_h, ge), (ue_h, ue),
            (gl_h, gl), (ul_h, ul), (gin_h, gin),
        )
        return pltpu.make_async_copy(pairs[i][0], pairs[i][1], ld.at[i])

    for i in range(4):
        loads(i).start()

    barrier = pltpu.get_barrier_semaphore()

    @pl.when(z < nz - 1)
    def _():
        pl.semaphore_signal(barrier, inc=1, device_id={"fs": me + 2}, device_id_type=MESH)

    @pl.when(z > 0)
    def _():
        pl.semaphore_signal(barrier, inc=1, device_id={"fs": me - 2}, device_id_type=MESH)

    pl.semaphore_signal(barrier, inc=1, device_id={"fs": 2 * z + 1 - y}, device_id_type=MESH)
    pl.semaphore_signal(barrier, inc=1, device_id={"rep": other}, device_id_type=MESH)
    for k in range(1, n_tp):
        pl.semaphore_signal(barrier, inc=1, device_id={"tp": lax.rem(tp + k, n_tp)}, device_id_type=MESH)
    inner = jnp.where((z > 0) & (z < nz - 1), 1, 0)
    pl.semaphore_wait(barrier, 2 + n_tp + inner)

    def target(way):
        if way == RIGHT:
            return {"fs": me + 2}
        if way == LEFT:
            return {"fs": me - 2}
        if way == ACROSS:
            return {"fs": 2 * z + 1 - y}
        return {"rep": other}

    def piece_rows(p):
        size = (quarter, third, rows - 2 * quarter - third, quarter)[p]
        start = (0, quarter, quarter + third, rows - quarter)[p]
        return pl.ds(pl.multiple_of(start + rep * (rows - 2 * start - size), 16), size)

    def piece(way, shard, p):
        spot = wf.at[shard, piece_rows(p), :]
        return pltpu.make_async_remote_copy(
            src_ref=spot, dst_ref=spot, send_sem=ag_s.at[way, shard, p],
            recv_sem=ag_r.at[shard, 3 if way == OTHER else p],
            device_id=target(way), device_id_type=MESH,
        )

    def piece_arrived(shard, p):
        spot = wf.at[shard, piece_rows(p), :]
        pltpu.make_async_remote_copy(
            src_ref=spot, dst_ref=spot, send_sem=ag_s.at[0, shard, 0], recv_sem=ag_r.at[shard, p],
            device_id=target(OTHER), device_id_type=MESH,
        ).wait_recv()

    loads(0).wait()
    for p in range(3):
        if p < 2 or YI < 0:
            piece(ACROSS, me, (2, 0, 1)[p]).start()

        @pl.when(z < nz - 1)
        def _():
            piece(RIGHT, me, p).start()

        @pl.when(z > 0)
        def _():
            piece(LEFT, me, p).start()

    def nearest(m):
        low = jnp.minimum(z, nz - 1 - z)
        paired = m <= 2 * low
        step = jnp.where(paired, lax.div(m + 1, 2), m - low)
        down = jnp.where(paired, lax.rem(m, 2) == 1, 2 * z > nz - 1)
        return jnp.where(down, z - step, z + step)

    for i in range(4, 7):
        loads(i).start()

    lot = tokens // n_tp

    def cot_piece(start, to):
        span = pl.ds(pl.multiple_of(start, 16), lot)
        if flat:
            return cot.at[span, pl.ds(pl.multiple_of(2 * to * rows, 2 * rows), 2 * rows)]
        return cot.at[pl.ds(2 * to, 2), span, :]

    def cot_cross(to):
        return pltpu.make_async_remote_copy(
            src_ref=cot_piece(tp * lot, to), dst_ref=cot_piece(tokens + tp * lot, to),
            send_sem=cx_s.at[to], recv_sem=cx_r.at[to],
            device_id={"rep": other}, device_id_type=MESH,
        )

    def cot_share(k, sender, to):
        spot = cot_piece(tokens + sender * lot, to)
        return pltpu.make_async_remote_copy(
            src_ref=spot, dst_ref=spot, send_sem=ct_s.at[k, to], recv_sem=ct_r.at[k, to],
            device_id={"tp": lax.rem(tp + k, n_tp)}, device_id_type=MESH,
        )

    loads(1).wait()
    cot_cross(nearest(nz - 1)).start()

    def columns(c):
        return pl.ds(pl.multiple_of(c * width, 128), width)

    def he_cross(c):
        return pltpu.make_async_remote_copy(
            src_ref=he_out.at[:, columns(c)], dst_ref=he.at[pl.ds(tokens, tokens), columns(c)],
            send_sem=he_s.at[c], recv_sem=he_r.at[c], device_id={"rep": other}, device_id_type=MESH,
        )

    def tile_at(i):
        return pl.ds(pl.multiple_of(i * TILE, TILE), TILE)

    def gated(gate_ref, up_ref, span, lanes):
        gate = gate_ref[span, lanes].astype(F32)
        return (gate * (1.0 / (1.0 + jnp.exp(-gate))) * up_ref[span, lanes].astype(F32)).astype(BF16)

    mine_lanes = pl.ds(pl.multiple_of(rep * hq, 128), hq)
    theirs_lanes = pl.ds(pl.multiple_of(other * hq, 128), hq)
    loads(2).wait()
    loads(3).wait()

    @pl.loop(0, tokens // TILE)
    def _(i):
        he_out[tile_at(i), :] = gated(ge, ue, tile_at(i), theirs_lanes)

    he_cross(0).start()

    @pl.loop(1, nz)
    def _(m):
        cot_cross(nearest(nz - 1 - m)).start()

    for c in range(1, chunks):
        he_cross(c).start()

    @pl.loop(0, tokens // TILE)
    def _(i):
        he[tile_at(i), :] = gated(ge, ue, tile_at(i), mine_lanes)

    beyond = 2 * z + 1 - y
    piece_arrived(beyond, 2)

    @pl.when(z < nz - 1)
    def _():
        piece(RIGHT, beyond, 2).start()

    @pl.when(z > 0)
    def _():
        piece(LEFT, beyond, 2).start()

    loads(4).wait()
    loads(5).wait()

    @pl.loop(0, tokens // TILE)
    def _(i):
        hl[tile_at(i), :] = gated(gl, ul, tile_at(i), slice(None))
        hg[tile_at(i), :] = jnp.zeros((TILE, cols), F32)

    def onward(k, arrive, pass_on):
        hop = lax.div(k, 4) + 1
        for p in range(4):
            line = 1 - y if p == 3 else y
            q = 2 if p == 3 else p
            for source, step, way in ((z - hop, 1, RIGHT), (z + hop, -1, LEFT)):
                shard = 2 * source + line

                @pl.when((lax.rem(k, 4) == p) & (source >= 0) & (source < nz))
                def _():
                    if arrive:
                        piece_arrived(shard, q)

                    @pl.when((z + step >= 0) & (z + step < nz) & pass_on(hop))
                    def _():
                        piece(way, shard, q).start()

                    if arrive and p == 0:
                        if Y0 == 0:
                            piece(ACROSS, shard, 0).start()
                        piece(OTHER, shard, 0).start()

    def gather(k):
        onward(k, True, lambda hop: (hop < 2) | (HOLD == 0))

    def held(k):
        onward(k, False, lambda hop: hop >= 2)

    def across(k, p):
        hop = lax.div(k, 4) + 1
        for source in (z - hop, z + hop):

            @pl.when((source >= 0) & (source < nz))
            def _():
                piece(ACROSS, 2 * source + y, p).start()

    def gather_across(k):
        hop = lax.div(k, 4) + 1
        for source in (z - hop, z + hop):

            @pl.when((source >= 0) & (source < nz))
            def _():
                shard = 2 * source + 1 - y
                piece_arrived(shard, 0)
                piece(OTHER, shard, 0).start()

    def cot_block(first, size, shard):
        if flat:
            return cot[pl.ds(first, size), pl.ds(pl.multiple_of(shard * rows, rows), rows)]
        return cot[shard, pl.ds(first, size), :]

    def share(k, shard):
        return pltpu.make_async_remote_copy(
            src_ref=part.at[tp, shard], dst_ref=part.at[tp, shard],
            send_sem=tp_s.at[k, shard], recv_sem=tp_r.at[k, shard],
            device_id={"tp": lax.rem(tp + k, n_tp)}, device_id_type=MESH,
        )

    def share_arrived(k, shard):
        spot = part.at[lax.rem(tp + n_tp - k, n_tp), shard]
        pltpu.make_async_remote_copy(
            src_ref=spot, dst_ref=spot, send_sem=tp_s.at[k, shard], recv_sem=tp_r.at[k, shard],
            device_id={"tp": lax.rem(tp + k, n_tp)}, device_id_type=MESH,
        ).wait_recv()

    def use(i, carry):
        crossed = lax.rem(i, 2)
        line = jnp.where(crossed == 1, 1 - y, y)
        shard = 2 * nearest(lax.div(i, 2)) + line

        @pl.when(crossed == 1)
        def _():
            piece_arrived(shard, 1)

        @pl.when(i > 0)
        def _():
            piece_arrived(shard, 3)

        block = wf[shard]
        part[tp, shard] = lax.dot_general(
            hl[...], block, (((1,), (1,)), ((), ())), preferred_element_type=F32
        ).astype(BF16)
        for k in range(1, n_tp):
            share(k, shard).start()
        hg[...] += jnp.dot(cot_block(0, tokens, shard), block, preferred_element_type=F32)
        return carry

    def y_copy(c, to):
        return pltpu.make_async_remote_copy(
            src_ref=ys.at[c, to], dst_ref=yr.at[c, to], send_sem=y_s.at[c, to], recv_sem=y_r.at[c, to],
            device_id=target(ACROSS), device_id_type=MESH,
        )

    first, second = halves = pl.ds(0, head), pl.ds(head, tail)
    mine, cross = pl.ds(0, tail), pl.ds(tail, tail)
    bulk = pl.ds(0, 2 * tail)
    rest = pl.ds(2 * tail, head)

    def z_copy(way, c, to, stage, towards=None):
        span = (bulk, rest)[stage]
        return pltpu.make_async_remote_copy(
            src_ref=zs.at[c, to, span, :], dst_ref=zr.at[way, c, to, span, :],
            send_sem=z_s.at[stage, c, to], recv_sem=z_r.at[2 * way + stage, c, to],
            device_id=target(way if towards is None else towards), device_id_type=MESH,
        )

    def z_arrived(way, c, to, stage):
        z_copy(way, c, to, stage, OTHER).wait_recv()

    def yf_copy(c):
        return pltpu.make_async_remote_copy(
            src_ref=yfs.at[c], dst_ref=yfr.at[c], send_sem=yf_s.at[c], recv_sem=yf_r.at[c],
            device_id=target(ACROSS), device_id_type=MESH,
        )

    def x_copy(c, stage):
        return pltpu.make_async_remote_copy(
            src_ref=xs.at[c, halves[stage], :], dst_ref=xr.at[c, halves[stage], :],
            send_sem=x_s.at[stage, c], recv_sem=x_r.at[stage, c],
            device_id={"rep": other}, device_id_type=MESH,
        )

    def contribute(c, m):
        to = nearest(nz - 1 - m)

        @pl.when(c == 0)
        def _():
            cot_cross(to).wait_recv()
            for k in range(1, n_tp):
                cot_share(k, tp, to).start()

        @pl.when(m == 0)
        def _():
            he_cross(c).wait_recv()

        @pl.when(c == 0)
        def _():
            for k in range(1, n_tp):
                cot_share(k, lax.rem(tp + n_tp - k, n_tp), to).wait_recv()

        def term(line):
            return lax.dot_general(
                cot_block(0, 2 * tokens, 2 * to + line), he[:, columns(c)],
                (((0,), (0,)), ((), ())), preferred_element_type=F32,
            )

        value = term(1 - y)
        ys[c, to] = value[:head].astype(BF16)
        y_copy(c, to).start()
        opp[c, to] = value[head:]
        own[c, to] = term(y)


    def forward(s):
        for way, place in ((RIGHT, z), (LEFT, nz - 1 - z)):
            at = s + jnp.where(place == 0, LEAD, 0)
            safe = jnp.maximum(at, 0)
            c = lax.div(safe, nz - 1)
            j = lax.rem(safe, nz - 1) - place

            @pl.when((at >= 0) & (at < chunks * (nz - 1)) & (j >= 0))
            def _():
                to = nz - 1 - j if way == RIGHT else j

                @pl.when(place == 0)
                def _():
                    zs[c, to, mine, :] = own[c, to, second, :].astype(BF16)
                    zs[c, to, cross, :] = opp[c, to].astype(BF16)

                @pl.when(place > 0)
                def _():
                    z_arrived(way, c, to, 0)
                    before = zr.at[way, c, to]
                    zs[c, to, mine, :] = (own[c, to, second, :] + before[mine, :].astype(F32)).astype(BF16)
                    zs[c, to, cross, :] = (opp[c, to] + before[cross, :].astype(F32)).astype(BF16)

                z_copy(way, c, to, 0).start()

    def forward_rest(s):
        for way, place in ((RIGHT, z), (LEFT, nz - 1 - z)):
            at = s + jnp.where(place == 0, LEAD, 0)
            safe = jnp.maximum(at, 0)
            c = lax.div(safe, nz - 1)
            j = lax.rem(safe, nz - 1) - place

            @pl.when((at >= 0) & (at < chunks * (nz - 1)) & (j >= 0))
            def _():
                to = nz - 1 - j if way == RIGHT else j
                y_copy(c, to).wait_recv()

                @pl.when(place == 0)
                def _():
                    zs[c, to, rest, :] = (own[c, to, first, :] + yr[c, to].astype(F32)).astype(BF16)

                @pl.when(place > 0)
                def _():
                    z_arrived(way, c, to, 1)
                    zs[c, to, rest, :] = (
                        own[c, to, first, :] + yr[c, to].astype(F32) + zr[way, c, to, rest, :].astype(F32)
                    ).astype(BF16)

                z_copy(way, c, to, 1).start()

    sides = ((RIGHT, z > 0), (LEFT, z < nz - 1))

    def finish_line(c):
        for way, there in sides:

            @pl.when(there)
            def _():
                z_arrived(way, c, z, 0)
                before = zr.at[way, c, z]
                opp[c, z] += before[cross, :].astype(F32)
                own[c, z, second, :] += before[mine, :].astype(F32)

        yfs[c] = opp[c, z].astype(BF16)
        yf_copy(c).start()
        y_copy(c, z).wait_recv()
        own[c, z, first, :] += yr[c, z].astype(F32)
        for way, there in sides:

            @pl.when(there)
            def _():
                z_arrived(way, c, z, 1)
                own[c, z, first, :] += zr[way, c, z, rest, :].astype(F32)

        xs[c, first, :] = own[c, z, first, :].astype(BF16)
        x_copy(c, 0).start()

    def finish_pair(c):
        yf_copy(c).wait_recv()
        own[c, z, second, :] += yfr[c].astype(F32)
        xs[c, second, :] = own[c, z, second, :].astype(BF16)
        x_copy(c, 1).start()
        lanes = pl.ds(pl.multiple_of(rep * hq + c * width, 128), width)
        gout[:, lanes] = gin[:, lanes] + own[c, z] * scale

    def finish_cross(c):
        lanes = pl.ds(pl.multiple_of(other * hq + c * width, 128), width)
        for stage, span in ((0, first), (1, second)):
            x_copy(c, stage).wait_recv()
            gout[span, lanes] = gin[span, lanes] + xr[c, span, :].astype(F32) * scale

    def reduce_step(s):
        def when_due(offset, ready, act):
            at = s - offset
            safe = jnp.maximum(at, 0)
            c = lax.div(safe, nz - 1) + ready

            @pl.when((at >= 0) & (lax.rem(safe, nz - 1) == 0) & (c >= 0) & (c < chunks))
            def _():
                act(c)

        base = s + lead + ahead

        @pl.loop(0, 2)
        def _(turn):
            late_turn = 1 - turn
            c = lax.div(base, nz - 1) - late_turn
            m = lax.rem(base, nz - 1) + late_turn * (nz - 1)

            @pl.when((m < nz) & (c >= 0) & (c < chunks))
            def _():
                contribute(c, m)

        forward(s)
        forward_rest(s - split)
        when_due(settle, -1, finish_line)
        when_due(pair_due, -1, finish_pair)
        when_due(cross_due, -1, finish_cross)

    gather_ticks = 4 * (nz - 1)
    use_ticks = max(2 * n - 3, n + max(USE_LAG))
    last_step = chunks * (nz - 1) + cross_due
    sum_ticks = max(
        START[i] + chunks * (nz - 1) + LEAD + AHEAD[i] + SETTLE[i] + FP[i] + FC[i] for i in range(2)
    )

    def used(k):
        return jnp.clip(jnp.minimum(lax.div(k + 2, 2), k - use_lag) + 1, 1, n)

    def reduce_tick(k):
        step = k - begin - lead - ahead

        @pl.when((k >= begin) & (step < last_step))
        def _():
            reduce_step(step)

    def when_gathering(k, act, *more):
        @pl.when((k >= 0) & (k < gather_ticks) & functools.reduce(jnp.logical_and, more, True))
        def _():
            act(k)

    def tick(k, carry):
        if RSFIRST == 1:
            reduce_tick(k)
        when_gathering(k, gather)
        behind = k - lag
        when_gathering(behind, gather_across, lax.rem(jnp.maximum(behind, 0), 4) == 0)

        @pl.when(k == 1)
        def _():
            piece_arrived(beyond, 0)
            piece(OTHER, beyond, 0).start()

        @pl.when(k == max(START))
        def _():
            loads(6).wait()

        if RSFIRST == 0:
            reduce_tick(k)
        if Y0 > 0:
            at = k - Y0
            when_gathering(at, lambda j: across(j, 0), lax.rem(jnp.maximum(at, 0), 4) == 0)
        at = k - Y1
        when_gathering(at, lambda j: across(j, 1), lax.rem(jnp.maximum(at, 0), 4) == 1, (at < 4) | (Y1H == 0))
        if Y1H:
            when_gathering(k, lambda j: across(j, 1), lax.rem(k, 4) == 1, k >= 4)
        if HOLD:
            when_gathering(k - HOLD, held)
        if YI >= 0:

            @pl.when(k == YI)
            def _():
                piece(ACROSS, me, 1).start()

        if RSFIRST == 2:
            reduce_tick(k)
        lax.fori_loop(jnp.where(k == 0, 0, used(k - 1)), used(k), use, 0)
        return carry

    lax.fori_loop(0, max(use_ticks, gather_ticks, sum_ticks), tick, 0)

    @pl.loop(0, tokens // TILE)
    def _(i):
        span = tile_at(i)
        gate = ge[span, :].astype(F32)
        sig = 1.0 / (1.0 + jnp.exp(-gate))
        grad = hg[span, :]
        ug[span, :] = (grad * (gate * sig)).astype(BF16)
        gg[span, :] = (
            grad * ue[span, :].astype(F32) * sig * (1.0 + gate * (1.0 - sig))
        ).astype(BF16)

    @pl.loop(0, n)
    def _(shard):
        for k in range(1, n_tp):
            share_arrived(k, shard)
        total = part[0, shard].astype(F32)
        for j in range(1, n_tp):
            total = total + part[j, shard].astype(F32)
        if flat:
            late[:, pl.ds(pl.multiple_of(shard * rows, rows), rows)] = total.astype(BF16)
        else:
            late[shard] = total.astype(BF16)

    reduce_step(jnp.int32(last_step))

    for p in range(3):
        piece(ACROSS, me, p).wait_send()

    @pl.loop(0, nz)
    def _(at):
        same = 2 * at + y
        crossed = 2 * at + 1 - y

        @pl.when((at <= z) & (z < nz - 1))
        def _():
            for p in range(3):
                piece(RIGHT, same, p).wait_send()
            piece(RIGHT, crossed, 2).wait_send()

        @pl.when((at >= z) & (z > 0))
        def _():
            for p in range(3):
                piece(LEFT, same, p).wait_send()
            piece(LEFT, crossed, 2).wait_send()

        piece(OTHER, crossed, 0).wait_send()
        cot_cross(at).wait_send()

        @pl.when(at != z)
        def _():
            piece(OTHER, same, 0).wait_send()
            for p in range(2):
                piece(ACROSS, same, p).wait_send()

        for k in range(1, n_tp):
            cot_share(k, tp, at).wait_send()
            share(k, same).wait_send()
            share(k, crossed).wait_send()

        @pl.loop(0, chunks)
        def _(c):
            y_copy(c, at).wait_send()

            @pl.when(at > z)
            def _():
                z_copy(RIGHT, c, at, 0).wait_send()
                z_copy(RIGHT, c, at, 1).wait_send()

            @pl.when(at < z)
            def _():
                z_copy(LEFT, c, at, 0).wait_send()
                z_copy(LEFT, c, at, 1).wait_send()

    @pl.loop(0, chunks)
    def _(c):
        he_cross(c).wait_send()
        yf_copy(c).wait_send()
        x_copy(c, 0).wait_send()
        x_copy(c, 1).wait_send()


def deliver(*refs):
    count = 4
    sems = refs[-1]
    copies = [
        pltpu.make_async_copy(refs[i], refs[count + i], sems.at[i]) for i in range(count)
    ]
    for copy in copies:
        copy.start()
    for copy in copies:
        copy.wait()


def solution(mesh):
    n, n_tp, n_rep = mesh.shape["fs"], mesh.shape["tp"], mesh.shape["rep"]
    assert n_rep == 2 and n % 2 == 0 and n >= 8

    def per_device(gl, ul, ge, ue, cotangent, w, gin):
        tokens, cols = gl.shape
        rows, width = w.shape[0], cotangent.shape[1]
        assert rows % 64 == 0 and cols % 256 == 0
        nz, hq = n // 2, cols // 2
        head = max(rows * H0 // 256, 1) * 16
        tail = rows - head
        chunks = min(CHUNKS, hq // 128)
        scale = 1.0 / math.sqrt(tokens * n_rep * n)
        whole_lanes = rows % 128 == 0
        cot = cotangent
        if not whole_lanes:
            cot = cotangent.reshape(tokens, n, rows).transpose(1, 0, 2)
        cot_both = (2 * tokens, width) if whole_lanes else (n, 2 * tokens, rows)
        vmem = pl.BlockSpec(memory_space=pltpu.VMEM)
        dma = pltpu.SemaphoreType.DMA
        part = hq // chunks
        late, gg, ug, gout = pl.pallas_call(
            functools.partial(kernel, n, n_tp, chunks, scale),
            out_shape=(
                pltpu.VMEM(cot.shape, BF16),
                pltpu.VMEM((tokens, cols), BF16),
                pltpu.VMEM((tokens, cols), BF16),
                pltpu.VMEM((rows, cols), F32),
            ),
            in_specs=[pl.BlockSpec(memory_space=pl.ANY)] * 7,
            out_specs=(vmem,) * 4,
            scratch_shapes=[
                pltpu.VMEM((tokens, cols), BF16),
                pltpu.VMEM((tokens, cols), BF16),
                pltpu.VMEM((tokens, cols), BF16),
                pltpu.VMEM((tokens, cols), BF16),
                pltpu.VMEM(cot_both, BF16),
                pltpu.VMEM((rows, cols), F32),
                pltpu.VMEM((n, rows, cols), BF16),
                pltpu.VMEM((tokens, cols), BF16),
                pltpu.VMEM((2 * tokens, hq), BF16),
                pltpu.VMEM((tokens, hq), BF16),
                pltpu.VMEM((tokens, cols), F32),
                pltpu.VMEM((n_tp, n, tokens, rows), BF16),
                pltpu.VMEM((chunks, nz, rows, part), F32),
                pltpu.VMEM((chunks, nz, tail, part), F32),
                pltpu.VMEM((chunks, nz, head, part), BF16),
                pltpu.VMEM((chunks, nz, head, part), BF16),
                pltpu.VMEM((chunks, nz, rows + tail, part), BF16),
                pltpu.VMEM((2, chunks, nz, rows + tail, part), BF16),
                pltpu.VMEM((chunks, tail, part), BF16),
                pltpu.VMEM((chunks, tail, part), BF16),
                pltpu.VMEM((chunks, rows, part), BF16),
                pltpu.VMEM((chunks, rows, part), BF16),
                dma((7,)),
                dma((4, n, 3)),
                dma((n, 4)),
                dma((nz,)),
                dma((nz,)),
                dma((n_tp, nz)),
                dma((n_tp, nz)),
                dma((chunks,)),
                dma((chunks,)),
                dma((chunks, nz)),
                dma((chunks, nz)),
                dma((2, chunks, nz)),
                dma((4, chunks, nz)),
                dma((chunks,)),
                dma((chunks,)),
                dma((2, chunks)),
                dma((2, chunks)),
                dma((n_tp, n)),
                dma((n_tp, n)),
            ],
            compiler_params=pltpu.CompilerParams(
                collective_id=0, has_side_effects=True, vmem_limit_bytes=LIMIT
            ),
        )(gl, ul, ge, ue, cot, w, gin)
        late, gg, ug, gout = pl.pallas_call(
            deliver,
            out_shape=tuple(jax.ShapeDtypeStruct(a.shape, a.dtype) for a in (late, gg, ug, gout)),
            in_specs=[pl.BlockSpec(memory_space=pl.ANY)] * 4,
            out_specs=(pl.BlockSpec(memory_space=pl.ANY),) * 4,
            scratch_shapes=[dma((4,))],
            compiler_params=pltpu.CompilerParams(vmem_limit_bytes=1 << 20),
        )(late, gg, ug, gout)
        if not whole_lanes:
            late = late.transpose(1, 0, 2).reshape(tokens, width)
        return late, gg, ug, gout

    placed = (
        P(("rep", "fs"), "tp"),
        P(("rep", "fs"), "tp"),
        P(("rep", "fs"), "tp"),
        P(("rep", "fs"), "tp"),
        P(("rep", "fs"), None),
        P("fs", "tp"),
        P("fs", "tp"),
    )
    return jax.shard_map(
        per_device,
        mesh=mesh,
        in_specs=placed,
        out_specs=(
            P(("rep", "fs"), None),
            P(("rep", "fs"), "tp"),
            P(("rep", "fs"), "tp"),
            P("fs", "tp"),
        ),
        check_vma=False,
    )
```

```python
import functools
import math

import jax
import jax.numpy as jnp
from jax import lax
from jax.experimental import pallas as pl
from jax.experimental.pallas import tpu as pltpu
from jax.sharding import PartitionSpec as P

MESH = pl.DeviceIdType.MESH
F32 = jnp.float32
BF16 = jnp.bfloat16
RIGHT, LEFT, ACROSS, OTHER = 0, 1, 2, 3
LIMIT = 56 << 20
CHUNKS = 2
LEAD = 2
AHEAD = (1, 1)
SETTLE = (2, 0)
START = (2, 1)
LAG = (4, 4)
USE_LAG = (7, 5)
Y0 = 1
Y1 = 2
Y1H = 0
F1 = (0, 0)
RSFIRST = 1
YI = -1
HOLD = 0
FP = (2, 2)
FC = (1, 1)
P1 = 6
H0 = 6
TILE = 16


def kernel(
    n, n_tp, chunks, scale,
    gl_h, ul_h, ge_h, ue_h, cot_h, w_h, gin_h,
    late, gg, ug, gout,
    gl, ul, ge, ue, cot, gin, wf, hl, he, he_out, hg, part, own, opp, ys, yr, zs, zr, yfs, yfr, xs, xr,
    ld, ag_s, ag_r, cx_s, cx_r, ct_s, ct_r, he_s, he_r, y_s, y_r, z_s, z_r, yf_s, yf_r, x_s, x_r, tp_s, tp_r,
):
    tokens, cols = gl.shape
    rows = wf.shape[1]
    quarter = rows // 4
    third = max(rows * P1 // 256, 1) * 16
    head = max(rows * H0 // 256, 1) * 16
    tail = rows - head
    nz = n // 2
    hq = cols // 2
    width = hq // chunks
    rep = lax.axis_index("rep")
    me = lax.axis_index("fs")
    tp = lax.axis_index("tp")
    z = lax.div(me, 2)
    y = lax.rem(me, 2)
    other = 1 - rep
    flat = len(cot.shape) == 2
    end = (z == 0) | (z == nz - 1)

    def pick(pair):
        return pair[0] if pair[0] == pair[1] else jnp.where(end, pair[0], pair[1])

    lead, ahead, settle = LEAD, pick(AHEAD), pick(SETTLE)
    begin, lag, use_lag, split = pick(START), pick(LAG), pick(USE_LAG), pick(F1)
    pair_due = settle + pick(FP)
    cross_due = pair_due + pick(FC)

    def cot_tokens(ref, start, size):
        return ref.at[pl.ds(start, size), :] if flat else ref.at[:, pl.ds(start, size), :]

    def loads(i):
        pairs = (
            (w_h, wf.at[me]), (cot_h, cot_tokens(cot, 0, tokens)), (ge_h, ge), (ue_h, ue),
            (gl_h, gl), (ul_h, ul), (gin_h, gin),
        )
        return pltpu.make_async_copy(pairs[i][0], pairs[i][1], ld.at[i])

    for i in range(4):
        loads(i).start()

    barrier = pltpu.get_barrier_semaphore()

    @pl.when(z < nz - 1)
    def _():
        pl.semaphore_signal(barrier, inc=1, device_id={"fs": me + 2}, device_id_type=MESH)

    @pl.when(z > 0)
    def _():
        pl.semaphore_signal(barrier, inc=1, device_id={"fs": me - 2}, device_id_type=MESH)

    pl.semaphore_signal(barrier, inc=1, device_id={"fs": 2 * z + 1 - y}, device_id_type=MESH)
    pl.semaphore_signal(barrier, inc=1, device_id={"rep": other}, device_id_type=MESH)
    for k in range(1, n_tp):
        pl.semaphore_signal(barrier, inc=1, device_id={"tp": lax.rem(tp + k, n_tp)}, device_id_type=MESH)
    inner = jnp.where((z > 0) & (z < nz - 1), 1, 0)
    pl.semaphore_wait(barrier, 2 + n_tp + inner)

    def target(way):
        if way == RIGHT:
            return {"fs": me + 2}
        if way == LEFT:
            return {"fs": me - 2}
        if way == ACROSS:
            return {"fs": 2 * z + 1 - y}
        return {"rep": other}

    def piece_rows(p):
        size = (quarter, third, rows - 2 * quarter - third, quarter)[p]
        start = (0, quarter, quarter + third, rows - quarter)[p]
        return pl.ds(pl.multiple_of(start + rep * (rows - 2 * start - size), 16), size)

    def piece(way, shard, p):
        spot = wf.at[shard, piece_rows(p), :]
        return pltpu.make_async_remote_copy(
            src_ref=spot, dst_ref=spot, send_sem=ag_s.at[way, shard, p],
            recv_sem=ag_r.at[shard, 3 if way == OTHER else p],
            device_id=target(way), device_id_type=MESH,
        )

    def piece_arrived(shard, p):
        spot = wf.at[shard, piece_rows(p), :]
        pltpu.make_async_remote_copy(
            src_ref=spot, dst_ref=spot, send_sem=ag_s.at[0, shard, 0], recv_sem=ag_r.at[shard, p],
            device_id=target(OTHER), device_id_type=MESH,
        ).wait_recv()

    loads(0).wait()
    for p in range(3):
        if p < 2 or YI < 0:
            piece(ACROSS, me, (2, 0, 1)[p]).start()

        @pl.when(z < nz - 1)
        def _():
            piece(RIGHT, me, p).start()

        @pl.when(z > 0)
        def _():
            piece(LEFT, me, p).start()

    def nearest(m):
        low = jnp.minimum(z, nz - 1 - z)
        paired = m <= 2 * low
        step = jnp.where(paired, lax.div(m + 1, 2), m - low)
        down = jnp.where(paired, lax.rem(m, 2) == 1, 2 * z > nz - 1)
        return jnp.where(down, z - step, z + step)

    for i in range(4, 7):
        loads(i).start()

    lot = tokens // n_tp

    def cot_piece(start, to):
        span = pl.ds(pl.multiple_of(start, 16), lot)
        if flat:
            return cot.at[span, pl.ds(pl.multiple_of(2 * to * rows, 2 * rows), 2 * rows)]
        return cot.at[pl.ds(2 * to, 2), span, :]

    def cot_cross(to):
        return pltpu.make_async_remote_copy(
            src_ref=cot_piece(tp * lot, to), dst_ref=cot_piece(tokens + tp * lot, to),
            send_sem=cx_s.at[to], recv_sem=cx_r.at[to],
            device_id={"rep": other}, device_id_type=MESH,
        )

    def cot_share(k, sender, to):
        spot = cot_piece(tokens + sender * lot, to)
        return pltpu.make_async_remote_copy(
            src_ref=spot, dst_ref=spot, send_sem=ct_s.at[k, to], recv_sem=ct_r.at[k, to],
            device_id={"tp": lax.rem(tp + k, n_tp)}, device_id_type=MESH,
        )

    loads(1).wait()
    cot_cross(nearest(nz - 1)).start()

    def columns(c):
        return pl.ds(pl.multiple_of(c * width, 128), width)

    def he_cross(c):
        return pltpu.make_async_remote_copy(
            src_ref=he_out.at[:, columns(c)], dst_ref=he.at[pl.ds(tokens, tokens), columns(c)],
            send_sem=he_s.at[c], recv_sem=he_r.at[c], device_id={"rep": other}, device_id_type=MESH,
        )

    def tile_at(i):
        return pl.ds(pl.multiple_of(i * TILE, TILE), TILE)

    def gated(gate_ref, up_ref, span, lanes):
        gate = gate_ref[span, lanes].astype(F32)
        return (gate * (1.0 / (1.0 + jnp.exp(-gate))) * up_ref[span, lanes].astype(F32)).astype(BF16)

    mine_lanes = pl.ds(pl.multiple_of(rep * hq, 128), hq)
    theirs_lanes = pl.ds(pl.multiple_of(other * hq, 128), hq)
    loads(2).wait()
    loads(3).wait()

    @pl.loop(0, tokens // TILE)
    def _(i):
        he_out[tile_at(i), :] = gated(ge, ue, tile_at(i), theirs_lanes)

    he_cross(0).start()

    @pl.loop(1, nz)
    def _(m):
        cot_cross(nearest(nz - 1 - m)).start()

    for c in range(1, chunks):
        he_cross(c).start()

    @pl.loop(0, tokens // TILE)
    def _(i):
        he[tile_at(i), :] = gated(ge, ue, tile_at(i), mine_lanes)

    beyond = 2 * z + 1 - y
    piece_arrived(beyond, 2)

    @pl.when(z < nz - 1)
    def _():
        piece(RIGHT, beyond, 2).start()

    @pl.when(z > 0)
    def _():
        piece(LEFT, beyond, 2).start()

    loads(4).wait()
    loads(5).wait()

    @pl.loop(0, tokens // TILE)
    def _(i):
        hl[tile_at(i), :] = gated(gl, ul, tile_at(i), slice(None))
        hg[tile_at(i), :] = jnp.zeros((TILE, cols), F32)

    def onward(k, arrive, pass_on):
        hop = lax.div(k, 4) + 1
        for p in range(4):
            line = 1 - y if p == 3 else y
            q = 2 if p == 3 else p
            for source, step, way in ((z - hop, 1, RIGHT), (z + hop, -1, LEFT)):
                shard = 2 * source + line

                @pl.when((lax.rem(k, 4) == p) & (source >= 0) & (source < nz))
                def _():
                    if arrive:
                        piece_arrived(shard, q)

                    @pl.when((z + step >= 0) & (z + step < nz) & pass_on(hop))
                    def _():
                        piece(way, shard, q).start()

                    if arrive and p == 0:
                        if Y0 == 0:
                            piece(ACROSS, shard, 0).start()
                        piece(OTHER, shard, 0).start()

    def gather(k):
        onward(k, True, lambda hop: (hop < 2) | (HOLD == 0))

    def held(k):
        onward(k, False, lambda hop: hop >= 2)

    def across(k, p):
        hop = lax.div(k, 4) + 1
        for source in (z - hop, z + hop):

            @pl.when((source >= 0) & (source < nz))
            def _():
                piece(ACROSS, 2 * source + y, p).start()

    def gather_across(k):
        hop = lax.div(k, 4) + 1
        for source in (z - hop, z + hop):

            @pl.when((source >= 0) & (source < nz))
            def _():
                shard = 2 * source + 1 - y
                piece_arrived(shard, 0)
                piece(OTHER, shard, 0).start()

    def cot_block(first, size, shard):
        if flat:
            return cot[pl.ds(first, size), pl.ds(pl.multiple_of(shard * rows, rows), rows)]
        return cot[shard, pl.ds(first, size), :]

    def share(k, shard):
        return pltpu.make_async_remote_copy(
            src_ref=part.at[tp, shard], dst_ref=part.at[tp, shard],
            send_sem=tp_s.at[k, shard], recv_sem=tp_r.at[k, shard],
            device_id={"tp": lax.rem(tp + k, n_tp)}, device_id_type=MESH,
        )

    def share_arrived(k, shard):
        spot = part.at[lax.rem(tp + n_tp - k, n_tp), shard]
        pltpu.make_async_remote_copy(
            src_ref=spot, dst_ref=spot, send_sem=tp_s.at[k, shard], recv_sem=tp_r.at[k, shard],
            device_id={"tp": lax.rem(tp + k, n_tp)}, device_id_type=MESH,
        ).wait_recv()

    def use(i, carry):
        crossed = lax.rem(i, 2)
        line = jnp.where(crossed == 1, 1 - y, y)
        shard = 2 * nearest(lax.div(i, 2)) + line

        @pl.when(crossed == 1)
        def _():
            piece_arrived(shard, 1)

        @pl.when(i > 0)
        def _():
            piece_arrived(shard, 3)

        block = wf[shard]
        part[tp, shard] = lax.dot_general(
            hl[...], block, (((1,), (1,)), ((), ())), preferred_element_type=F32
        ).astype(BF16)
        for k in range(1, n_tp):
            share(k, shard).start()
        hg[...] += jnp.dot(cot_block(0, tokens, shard), block, preferred_element_type=F32)
        return carry

    def y_copy(c, to):
        return pltpu.make_async_remote_copy(
            src_ref=ys.at[c, to], dst_ref=yr.at[c, to], send_sem=y_s.at[c, to], recv_sem=y_r.at[c, to],
            device_id=target(ACROSS), device_id_type=MESH,
        )

    first, second = halves = pl.ds(0, head), pl.ds(head, tail)
    mine, cross = pl.ds(0, tail), pl.ds(tail, tail)
    bulk = pl.ds(0, 2 * tail)
    rest = pl.ds(2 * tail, head)

    def z_copy(way, c, to, stage, towards=None):
        span = (bulk, rest)[stage]
        return pltpu.make_async_remote_copy(
            src_ref=zs.at[c, to, span, :], dst_ref=zr.at[way, c, to, span, :],
            send_sem=z_s.at[stage, c, to], recv_sem=z_r.at[2 * way + stage, c, to],
            device_id=target(way if towards is None else towards), device_id_type=MESH,
        )

    def z_arrived(way, c, to, stage):
        z_copy(way, c, to, stage, OTHER).wait_recv()

    def yf_copy(c):
        return pltpu.make_async_remote_copy(
            src_ref=yfs.at[c], dst_ref=yfr.at[c], send_sem=yf_s.at[c], recv_sem=yf_r.at[c],
            device_id=target(ACROSS), device_id_type=MESH,
        )

    def x_copy(c, stage):
        return pltpu.make_async_remote_copy(
            src_ref=xs.at[c, halves[stage], :], dst_ref=xr.at[c, halves[stage], :],
            send_sem=x_s.at[stage, c], recv_sem=x_r.at[stage, c],
            device_id={"rep": other}, device_id_type=MESH,
        )

    def contribute(c, m):
        to = nearest(nz - 1 - m)

        @pl.when(c == 0)
        def _():
            cot_cross(to).wait_recv()
            for k in range(1, n_tp):
                cot_share(k, tp, to).start()

        @pl.when(m == 0)
        def _():
            he_cross(c).wait_recv()

        @pl.when(c == 0)
        def _():
            for k in range(1, n_tp):
                cot_share(k, lax.rem(tp + n_tp - k, n_tp), to).wait_recv()

        def term(line):
            return lax.dot_general(
                cot_block(0, 2 * tokens, 2 * to + line), he[:, columns(c)],
                (((0,), (0,)), ((), ())), preferred_element_type=F32,
            )

        value = term(1 - y)
        ys[c, to] = value[:head].astype(BF16)
        y_copy(c, to).start()
        opp[c, to] = value[head:]
        own[c, to] = term(y)


    def forward(s):
        for way, place in ((RIGHT, z), (LEFT, nz - 1 - z)):
            at = s + jnp.where(place == 0, LEAD, 0)
            safe = jnp.maximum(at, 0)
            c = lax.div(safe, nz - 1)
            j = lax.rem(safe, nz - 1) - place

            @pl.when((at >= 0) & (at < chunks * (nz - 1)) & (j >= 0))
            def _():
                to = nz - 1 - j if way == RIGHT else j

                @pl.when(place == 0)
                def _():
                    zs[c, to, mine, :] = own[c, to, second, :].astype(BF16)
                    zs[c, to, cross, :] = opp[c, to].astype(BF16)

                @pl.when(place > 0)
                def _():
                    z_arrived(way, c, to, 0)
                    before = zr.at[way, c, to]
                    zs[c, to, mine, :] = (own[c, to, second, :] + before[mine, :].astype(F32)).astype(BF16)
                    zs[c, to, cross, :] = (opp[c, to] + before[cross, :].astype(F32)).astype(BF16)

                z_copy(way, c, to, 0).start()

    def forward_rest(s):
        for way, place in ((RIGHT, z), (LEFT, nz - 1 - z)):
            at = s + jnp.where(place == 0, LEAD, 0)
            safe = jnp.maximum(at, 0)
            c = lax.div(safe, nz - 1)
            j = lax.rem(safe, nz - 1) - place

            @pl.when((at >= 0) & (at < chunks * (nz - 1)) & (j >= 0))
            def _():
                to = nz - 1 - j if way == RIGHT else j
                y_copy(c, to).wait_recv()

                @pl.when(place == 0)
                def _():
                    zs[c, to, rest, :] = (own[c, to, first, :] + yr[c, to].astype(F32)).astype(BF16)

                @pl.when(place > 0)
                def _():
                    z_arrived(way, c, to, 1)
                    zs[c, to, rest, :] = (
                        own[c, to, first, :] + yr[c, to].astype(F32) + zr[way, c, to, rest, :].astype(F32)
                    ).astype(BF16)

                z_copy(way, c, to, 1).start()

    sides = ((RIGHT, z > 0), (LEFT, z < nz - 1))

    def finish_line(c):
        for way, there in sides:

            @pl.when(there)
            def _():
                z_arrived(way, c, z, 0)
                before = zr.at[way, c, z]
                opp[c, z] += before[cross, :].astype(F32)
                own[c, z, second, :] += before[mine, :].astype(F32)

        yfs[c] = opp[c, z].astype(BF16)
        yf_copy(c).start()
        y_copy(c, z).wait_recv()
        own[c, z, first, :] += yr[c, z].astype(F32)
        for way, there in sides:

            @pl.when(there)
            def _():
                z_arrived(way, c, z, 1)
                own[c, z, first, :] += zr[way, c, z, rest, :].astype(F32)

        xs[c, first, :] = own[c, z, first, :].astype(BF16)
        x_copy(c, 0).start()

    def finish_pair(c):
        yf_copy(c).wait_recv()
        own[c, z, second, :] += yfr[c].astype(F32)
        xs[c, second, :] = own[c, z, second, :].astype(BF16)
        x_copy(c, 1).start()
        lanes = pl.ds(pl.multiple_of(rep * hq + c * width, 128), width)
        gout[:, lanes] = gin[:, lanes] + own[c, z] * scale

    def finish_cross(c):
        lanes = pl.ds(pl.multiple_of(other * hq + c * width, 128), width)
        for stage, span in ((0, first), (1, second)):
            x_copy(c, stage).wait_recv()
            gout[span, lanes] = gin[span, lanes] + xr[c, span, :].astype(F32) * scale

    def reduce_step(s):
        def when_due(offset, ready, act):
            at = s - offset
            safe = jnp.maximum(at, 0)
            c = lax.div(safe, nz - 1) + ready

            @pl.when((at >= 0) & (lax.rem(safe, nz - 1) == 0) & (c >= 0) & (c < chunks))
            def _():
                act(c)

        base = s + lead + ahead

        @pl.loop(0, 2)
        def _(turn):
            late_turn = 1 - turn
            c = lax.div(base, nz - 1) - late_turn
            m = lax.rem(base, nz - 1) + late_turn * (nz - 1)

            @pl.when((m < nz) & (c >= 0) & (c < chunks))
            def _():
                contribute(c, m)

        forward(s)
        forward_rest(s - split)
        when_due(settle, -1, finish_line)
        when_due(pair_due, -1, finish_pair)
        when_due(cross_due, -1, finish_cross)

    gather_ticks = 4 * (nz - 1)
    use_ticks = max(2 * n - 3, n + max(USE_LAG))
    last_step = chunks * (nz - 1) + cross_due
    sum_ticks = max(
        START[i] + chunks * (nz - 1) + LEAD + AHEAD[i] + SETTLE[i] + FP[i] + FC[i] for i in range(2)
    )

    def used(k):
        return jnp.clip(jnp.minimum(lax.div(k + 2, 2), k - use_lag) + 1, 1, n)

    def reduce_tick(k):
        step = k - begin - lead - ahead

        @pl.when((k >= begin) & (step < last_step))
        def _():
            reduce_step(step)

    def when_gathering(k, act, *more):
        @pl.when((k >= 0) & (k < gather_ticks) & functools.reduce(jnp.logical_and, more, True))
        def _():
            act(k)

    def tick(k, carry):
        if RSFIRST == 1:
            reduce_tick(k)
        when_gathering(k, gather)
        behind = k - lag
        when_gathering(behind, gather_across, lax.rem(jnp.maximum(behind, 0), 4) == 0)

        @pl.when(k == 1)
        def _():
            piece_arrived(beyond, 0)
            piece(OTHER, beyond, 0).start()

        @pl.when(k == max(START))
        def _():
            loads(6).wait()

        if RSFIRST == 0:
            reduce_tick(k)
        if Y0 > 0:
            at = k - Y0
            when_gathering(at, lambda j: across(j, 0), lax.rem(jnp.maximum(at, 0), 4) == 0)
        at = k - Y1
        when_gathering(at, lambda j: across(j, 1), lax.rem(jnp.maximum(at, 0), 4) == 1, (at < 4) | (Y1H == 0))
        if Y1H:
            when_gathering(k, lambda j: across(j, 1), lax.rem(k, 4) == 1, k >= 4)
        if HOLD:
            when_gathering(k - HOLD, held)
        if YI >= 0:

            @pl.when(k == YI)
            def _():
                piece(ACROSS, me, 1).start()

        if RSFIRST == 2:
            reduce_tick(k)
        lax.fori_loop(jnp.where(k == 0, 0, used(k - 1)), used(k), use, 0)
        return carry

    lax.fori_loop(0, max(use_ticks, gather_ticks, sum_ticks), tick, 0)

    @pl.loop(0, tokens // TILE)
    def _(i):
        span = tile_at(i)
        gate = ge[span, :].astype(F32)
        sig = 1.0 / (1.0 + jnp.exp(-gate))
        grad = hg[span, :]
        ug[span, :] = (grad * (gate * sig)).astype(BF16)
        gg[span, :] = (
            grad * ue[span, :].astype(F32) * sig * (1.0 + gate * (1.0 - sig))
        ).astype(BF16)

    @pl.loop(0, n)
    def _(shard):
        for k in range(1, n_tp):
            share_arrived(k, shard)
        total = part[0, shard].astype(F32)
        for j in range(1, n_tp):
            total = total + part[j, shard].astype(F32)
        if flat:
            late[:, pl.ds(pl.multiple_of(shard * rows, rows), rows)] = total.astype(BF16)
        else:
            late[shard] = total.astype(BF16)

    reduce_step(jnp.int32(last_step))

    for p in range(3):
        piece(ACROSS, me, p).wait_send()

    @pl.loop(0, nz)
    def _(at):
        same = 2 * at + y
        crossed = 2 * at + 1 - y

        @pl.when((at <= z) & (z < nz - 1))
        def _():
            for p in range(3):
                piece(RIGHT, same, p).wait_send()
            piece(RIGHT, crossed, 2).wait_send()

        @pl.when((at >= z) & (z > 0))
        def _():
            for p in range(3):
                piece(LEFT, same, p).wait_send()
            piece(LEFT, crossed, 2).wait_send()

        piece(OTHER, crossed, 0).wait_send()
        cot_cross(at).wait_send()

        @pl.when(at != z)
        def _():
            piece(OTHER, same, 0).wait_send()
            for p in range(2):
                piece(ACROSS, same, p).wait_send()

        for k in range(1, n_tp):
            cot_share(k, tp, at).wait_send()
            share(k, same).wait_send()
            share(k, crossed).wait_send()

        @pl.loop(0, chunks)
        def _(c):
            y_copy(c, at).wait_send()

            @pl.when(at > z)
            def _():
                z_copy(RIGHT, c, at, 0).wait_send()
                z_copy(RIGHT, c, at, 1).wait_send()

            @pl.when(at < z)
            def _():
                z_copy(LEFT, c, at, 0).wait_send()
                z_copy(LEFT, c, at, 1).wait_send()

    @pl.loop(0, chunks)
    def _(c):
        he_cross(c).wait_send()
        yf_copy(c).wait_send()
        x_copy(c, 0).wait_send()
        x_copy(c, 1).wait_send()


def deliver(*refs):
    count = 4
    sems = refs[-1]
    copies = [
        pltpu.make_async_copy(refs[i], refs[count + i], sems.at[i]) for i in range(count)
    ]
    for copy in copies:
        copy.start()
    for copy in copies:
        copy.wait()


def solution(mesh):
    n, n_tp, n_rep = mesh.shape["fs"], mesh.shape["tp"], mesh.shape["rep"]
    assert n_rep == 2 and n % 2 == 0 and n >= 8

    def per_device(gl, ul, ge, ue, cotangent, w, gin):
        tokens, cols = gl.shape
        rows, width = w.shape[0], cotangent.shape[1]
        assert rows % 64 == 0 and cols % 256 == 0
        nz, hq = n // 2, cols // 2
        head = max(rows * H0 // 256, 1) * 16
        tail = rows - head
        chunks = min(CHUNKS, hq // 128)
        scale = 1.0 / math.sqrt(tokens * n_rep * n)
        whole_lanes = rows % 128 == 0
        cot = cotangent
        if not whole_lanes:
            cot = cotangent.reshape(tokens, n, rows).transpose(1, 0, 2)
        cot_both = (2 * tokens, width) if whole_lanes else (n, 2 * tokens, rows)
        vmem = pl.BlockSpec(memory_space=pltpu.VMEM)
        dma = pltpu.SemaphoreType.DMA
        part = hq // chunks
        late, gg, ug, gout = pl.pallas_call(
            functools.partial(kernel, n, n_tp, chunks, scale),
            out_shape=(
                pltpu.VMEM(cot.shape, BF16),
                pltpu.VMEM((tokens, cols), BF16),
                pltpu.VMEM((tokens, cols), BF16),
                pltpu.VMEM((rows, cols), F32),
            ),
            in_specs=[pl.BlockSpec(memory_space=pl.ANY)] * 7,
            out_specs=(vmem,) * 4,
            scratch_shapes=[
                pltpu.VMEM((tokens, cols), BF16),
                pltpu.VMEM((tokens, cols), BF16),
                pltpu.VMEM((tokens, cols), BF16),
                pltpu.VMEM((tokens, cols), BF16),
                pltpu.VMEM(cot_both, BF16),
                pltpu.VMEM((rows, cols), F32),
                pltpu.VMEM((n, rows, cols), BF16),
                pltpu.VMEM((tokens, cols), BF16),
                pltpu.VMEM((2 * tokens, hq), BF16),
                pltpu.VMEM((tokens, hq), BF16),
                pltpu.VMEM((tokens, cols), F32),
                pltpu.VMEM((n_tp, n, tokens, rows), BF16),
                pltpu.VMEM((chunks, nz, rows, part), F32),
                pltpu.VMEM((chunks, nz, tail, part), F32),
                pltpu.VMEM((chunks, nz, head, part), BF16),
                pltpu.VMEM((chunks, nz, head, part), BF16),
                pltpu.VMEM((chunks, nz, rows + tail, part), BF16),
                pltpu.VMEM((2, chunks, nz, rows + tail, part), BF16),
                pltpu.VMEM((chunks, tail, part), BF16),
                pltpu.VMEM((chunks, tail, part), BF16),
                pltpu.VMEM((chunks, rows, part), BF16),
                pltpu.VMEM((chunks, rows, part), BF16),
                dma((7,)),
                dma((4, n, 3)),
                dma((n, 4)),
                dma((nz,)),
                dma((nz,)),
                dma((n_tp, nz)),
                dma((n_tp, nz)),
                dma((chunks,)),
                dma((chunks,)),
                dma((chunks, nz)),
                dma((chunks, nz)),
                dma((2, chunks, nz)),
                dma((4, chunks, nz)),
                dma((chunks,)),
                dma((chunks,)),
                dma((2, chunks)),
                dma((2, chunks)),
                dma((n_tp, n)),
                dma((n_tp, n)),
            ],
            compiler_params=pltpu.CompilerParams(
                collective_id=0, has_side_effects=True, vmem_limit_bytes=LIMIT
            ),
        )(gl, ul, ge, ue, cot, w, gin)
        late, gg, ug, gout = pl.pallas_call(
            deliver,
            out_shape=tuple(jax.ShapeDtypeStruct(a.shape, a.dtype) for a in (late, gg, ug, gout)),
            in_specs=[pl.BlockSpec(memory_space=pl.ANY)] * 4,
            out_specs=(pl.BlockSpec(memory_space=pl.ANY),) * 4,
            scratch_shapes=[dma((4,))],
            compiler_params=pltpu.CompilerParams(vmem_limit_bytes=1 << 20),
        )(late, gg, ug, gout)
        if not whole_lanes:
            late = late.transpose(1, 0, 2).reshape(tokens, width)
        return late, gg, ug, gout

    placed = (
        P(("rep", "fs"), "tp"),
        P(("rep", "fs"), "tp"),
        P(("rep", "fs"), "tp"),
        P(("rep", "fs"), "tp"),
        P(("rep", "fs"), None),
        P("fs", "tp"),
        P("fs", "tp"),
    )
    return jax.shard_map(
        per_device,
        mesh=mesh,
        in_specs=placed,
        out_specs=(
            P(("rep", "fs"), None),
            P(("rep", "fs"), "tp"),
            P(("rep", "fs"), "tp"),
            P("fs", "tp"),
        ),
        check_vma=False,
    )
```

```python
import functools
import math

import jax
import jax.numpy as jnp
from jax import lax
from jax.experimental import pallas as pl
from jax.experimental.pallas import tpu as pltpu
from jax.sharding import PartitionSpec as P

MESH = pl.DeviceIdType.MESH
F32 = jnp.float32
BF16 = jnp.bfloat16
RIGHT, LEFT, ACROSS, OTHER = 0, 1, 2, 3
LIMIT = 56 << 20
CHUNKS = 2
LEAD = 2
AHEAD = (1, 1)
SETTLE = (2, 0)
START = (2, 1)
LAG = (4, 4)
USE_LAG = (7, 5)
Y0 = 1
Y1 = 2
Y1H = 0
F1 = (0, 0)
RSFIRST = 1
YI = -1
HOLD = 0
FP = (2, 2)
FC = (1, 1)
P1 = 6
H0 = 6
TILE = 16


def kernel(
    n, n_tp, chunks, scale,
    gl_h, ul_h, ge_h, ue_h, cot_h, w_h, gin_h,
    late, gg, ug, gout,
    gl, ul, ge, ue, cot, gin, wf, hl, he, he_out, hg, part, own, opp, ys, yr, zs, zr, yfs, yfr, xs, xr,
    ld, ag_s, ag_r, cx_s, cx_r, ct_s, ct_r, he_s, he_r, y_s, y_r, z_s, z_r, yf_s, yf_r, x_s, x_r, tp_s, tp_r,
):
    tokens, cols = gl.shape
    rows = wf.shape[1]
    quarter = rows // 4
    third = max(rows * P1 // 256, 1) * 16
    head = max(rows * H0 // 256, 1) * 16
    tail = rows - head
    cut = tail // 32 * 16
    cuts = pl.ds(0, cut), pl.ds(cut, tail - cut)
    nz = n // 2
    hq = cols // 2
    width = hq // chunks
    rep = lax.axis_index("rep")
    me = lax.axis_index("fs")
    tp = lax.axis_index("tp")
    z = lax.div(me, 2)
    y = lax.rem(me, 2)
    other = 1 - rep
    flat = len(cot.shape) == 2
    end = (z == 0) | (z == nz - 1)

    def pick(pair):
        return pair[0] if pair[0] == pair[1] else jnp.where(end, pair[0], pair[1])

    lead, ahead, settle = LEAD, pick(AHEAD), pick(SETTLE)
    begin, lag, use_lag, split = pick(START), pick(LAG), pick(USE_LAG), pick(F1)
    pair_due = settle + pick(FP)
    cross_due = pair_due + pick(FC)

    def cot_tokens(ref, start, size):
        return ref.at[pl.ds(start, size), :] if flat else ref.at[:, pl.ds(start, size), :]

    def loads(i):
        pairs = (
            (w_h, wf.at[me]), (cot_h, cot_tokens(cot, 0, tokens)), (ge_h, ge), (ue_h, ue),
            (gl_h, gl), (ul_h, ul), (gin_h, gin),
        )
        return pltpu.make_async_copy(pairs[i][0], pairs[i][1], ld.at[i])

    for i in range(4):
        loads(i).start()

    barrier = pltpu.get_barrier_semaphore()

    @pl.when(z < nz - 1)
    def _():
        pl.semaphore_signal(barrier, inc=1, device_id={"fs": me + 2}, device_id_type=MESH)

    @pl.when(z > 0)
    def _():
        pl.semaphore_signal(barrier, inc=1, device_id={"fs": me - 2}, device_id_type=MESH)

    pl.semaphore_signal(barrier, inc=1, device_id={"fs": 2 * z + 1 - y}, device_id_type=MESH)
    pl.semaphore_signal(barrier, inc=1, device_id={"rep": other}, device_id_type=MESH)
    for k in range(1, n_tp):
        pl.semaphore_signal(barrier, inc=1, device_id={"tp": lax.rem(tp + k, n_tp)}, device_id_type=MESH)
    inner = jnp.where((z > 0) & (z < nz - 1), 1, 0)
    pl.semaphore_wait(barrier, 2 + n_tp + inner)

    def target(way):
        if way == RIGHT:
            return {"fs": me + 2}
        if way == LEFT:
            return {"fs": me - 2}
        if way == ACROSS:
            return {"fs": 2 * z + 1 - y}
        return {"rep": other}

    def piece_rows(p):
        size = (quarter, third, rows - 2 * quarter - third, quarter)[p]
        start = (0, quarter, quarter + third, rows - quarter)[p]
        return pl.ds(pl.multiple_of(start + rep * (rows - 2 * start - size), 16), size)

    def piece(way, shard, p):
        spot = wf.at[shard, piece_rows(p), :]
        return pltpu.make_async_remote_copy(
            src_ref=spot, dst_ref=spot, send_sem=ag_s.at[way, shard, p],
            recv_sem=ag_r.at[shard, 3 if way == OTHER else p],
            device_id=target(way), device_id_type=MESH,
        )

    def piece_arrived(shard, p):
        spot = wf.at[shard, piece_rows(p), :]
        pltpu.make_async_remote_copy(
            src_ref=spot, dst_ref=spot, send_sem=ag_s.at[0, shard, 0], recv_sem=ag_r.at[shard, p],
            device_id=target(OTHER), device_id_type=MESH,
        ).wait_recv()

    loads(0).wait()
    for p in range(3):
        if p < 2 or YI < 0:
            piece(ACROSS, me, (2, 0, 1)[p]).start()

        @pl.when(z < nz - 1)
        def _():
            piece(RIGHT, me, p).start()

        @pl.when(z > 0)
        def _():
            piece(LEFT, me, p).start()

    def nearest(m):
        low = jnp.minimum(z, nz - 1 - z)
        paired = m <= 2 * low
        step = jnp.where(paired, lax.div(m + 1, 2), m - low)
        down = jnp.where(paired, lax.rem(m, 2) == 1, 2 * z > nz - 1)
        return jnp.where(down, z - step, z + step)

    for i in range(4, 7):
        loads(i).start()

    lot = tokens // n_tp

    def cot_piece(start, to):
        span = pl.ds(pl.multiple_of(start, 16), lot)
        if flat:
            return cot.at[span, pl.ds(pl.multiple_of(2 * to * rows, 2 * rows), 2 * rows)]
        return cot.at[pl.ds(2 * to, 2), span, :]

    def cot_cross(to):
        return pltpu.make_async_remote_copy(
            src_ref=cot_piece(tp * lot, to), dst_ref=cot_piece(tokens + tp * lot, to),
            send_sem=cx_s.at[to], recv_sem=cx_r.at[to],
            device_id={"rep": other}, device_id_type=MESH,
        )

    def cot_share(k, sender, to):
        spot = cot_piece(tokens + sender * lot, to)
        return pltpu.make_async_remote_copy(
            src_ref=spot, dst_ref=spot, send_sem=ct_s.at[k, to], recv_sem=ct_r.at[k, to],
            device_id={"tp": lax.rem(tp + k, n_tp)}, device_id_type=MESH,
        )

    loads(1).wait()
    cot_cross(nearest(nz - 1)).start()

    def columns(c):
        return pl.ds(pl.multiple_of(c * width, 128), width)

    def he_cross(c):
        return pltpu.make_async_remote_copy(
            src_ref=he_out.at[:, columns(c)], dst_ref=he.at[pl.ds(tokens, tokens), columns(c)],
            send_sem=he_s.at[c], recv_sem=he_r.at[c], device_id={"rep": other}, device_id_type=MESH,
        )

    def tile_at(i):
        return pl.ds(pl.multiple_of(i * TILE, TILE), TILE)

    def gated(gate_ref, up_ref, span, lanes):
        gate = gate_ref[span, lanes].astype(F32)
        return (gate * (1.0 / (1.0 + jnp.exp(-gate))) * up_ref[span, lanes].astype(F32)).astype(BF16)

    mine_lanes = pl.ds(pl.multiple_of(rep * hq, 128), hq)
    theirs_lanes = pl.ds(pl.multiple_of(other * hq, 128), hq)
    loads(2).wait()
    loads(3).wait()

    @pl.loop(0, tokens // TILE)
    def _(i):
        he_out[tile_at(i), :] = gated(ge, ue, tile_at(i), theirs_lanes)

    he_cross(0).start()

    @pl.loop(1, nz)
    def _(m):
        cot_cross(nearest(nz - 1 - m)).start()

    for c in range(1, chunks):
        he_cross(c).start()

    @pl.loop(0, tokens // TILE)
    def _(i):
        he[tile_at(i), :] = gated(ge, ue, tile_at(i), mine_lanes)

    beyond = 2 * z + 1 - y
    piece_arrived(beyond, 2)

    @pl.when(z < nz - 1)
    def _():
        piece(RIGHT, beyond, 2).start()

    @pl.when(z > 0)
    def _():
        piece(LEFT, beyond, 2).start()

    loads(4).wait()
    loads(5).wait()

    @pl.loop(0, tokens // TILE)
    def _(i):
        hl[tile_at(i), :] = gated(gl, ul, tile_at(i), slice(None))
        hg[tile_at(i), :] = jnp.zeros((TILE, cols), F32)

    def onward(k, arrive, pass_on):
        hop = lax.div(k, 4) + 1
        for p in range(4):
            line = 1 - y if p == 3 else y
            q = 2 if p == 3 else p
            for source, step, way in ((z - hop, 1, RIGHT), (z + hop, -1, LEFT)):
                shard = 2 * source + line

                @pl.when((lax.rem(k, 4) == p) & (source >= 0) & (source < nz))
                def _():
                    if arrive:
                        piece_arrived(shard, q)

                    @pl.when((z + step >= 0) & (z + step < nz) & pass_on(hop))
                    def _():
                        piece(way, shard, q).start()

                    if arrive and p == 0:
                        if Y0 == 0:
                            piece(ACROSS, shard, 0).start()
                        piece(OTHER, shard, 0).start()

    def gather(k):
        onward(k, True, lambda hop: (hop < 2) | (HOLD == 0))

    def held(k):
        onward(k, False, lambda hop: hop >= 2)

    def across(k, p):
        hop = lax.div(k, 4) + 1
        for source in (z - hop, z + hop):

            @pl.when((source >= 0) & (source < nz))
            def _():
                piece(ACROSS, 2 * source + y, p).start()

    def gather_across(k):
        hop = lax.div(k, 4) + 1
        for source in (z - hop, z + hop):

            @pl.when((source >= 0) & (source < nz))
            def _():
                shard = 2 * source + 1 - y
                piece_arrived(shard, 0)
                piece(OTHER, shard, 0).start()

    def cot_block(first, size, shard):
        if flat:
            return cot[pl.ds(first, size), pl.ds(pl.multiple_of(shard * rows, rows), rows)]
        return cot[shard, pl.ds(first, size), :]

    def share(k, shard):
        return pltpu.make_async_remote_copy(
            src_ref=part.at[tp, shard], dst_ref=part.at[tp, shard],
            send_sem=tp_s.at[k, shard], recv_sem=tp_r.at[k, shard],
            device_id={"tp": lax.rem(tp + k, n_tp)}, device_id_type=MESH,
        )

    def share_arrived(k, shard):
        spot = part.at[lax.rem(tp + n_tp - k, n_tp), shard]
        pltpu.make_async_remote_copy(
            src_ref=spot, dst_ref=spot, send_sem=tp_s.at[k, shard], recv_sem=tp_r.at[k, shard],
            device_id={"tp": lax.rem(tp + k, n_tp)}, device_id_type=MESH,
        ).wait_recv()

    def use(i, carry):
        crossed = lax.rem(i, 2)
        line = jnp.where(crossed == 1, 1 - y, y)
        shard = 2 * nearest(lax.div(i, 2)) + line

        @pl.when(crossed == 1)
        def _():
            piece_arrived(shard, 1)

        @pl.when(i > 0)
        def _():
            piece_arrived(shard, 3)

        block = wf[shard]
        part[tp, shard] = lax.dot_general(
            hl[...], block, (((1,), (1,)), ((), ())), preferred_element_type=F32
        ).astype(BF16)
        for k in range(1, n_tp):
            share(k, shard).start()
        hg[...] += jnp.dot(cot_block(0, tokens, shard), block, preferred_element_type=F32)
        return carry

    def y_copy(c, to):
        return pltpu.make_async_remote_copy(
            src_ref=ys.at[c, to], dst_ref=yr.at[c, to], send_sem=y_s.at[c, to], recv_sem=y_r.at[c, to],
            device_id=target(ACROSS), device_id_type=MESH,
        )

    first, second = pl.ds(0, head), pl.ds(head, tail)
    spans = first, pl.ds(head, cut), pl.ds(head + cut, tail - cut)
    mine, cross = pl.ds(0, tail), pl.ds(tail, tail)
    bulk = pl.ds(0, 2 * tail)
    rest = pl.ds(2 * tail, head)

    def z_copy(way, c, to, stage, towards=None):
        span = (bulk, rest)[stage]
        return pltpu.make_async_remote_copy(
            src_ref=zs.at[c, to, span, :], dst_ref=zr.at[way, c, to, span, :],
            send_sem=z_s.at[stage, c, to], recv_sem=z_r.at[2 * way + stage, c, to],
            device_id=target(way if towards is None else towards), device_id_type=MESH,
        )

    def z_arrived(way, c, to, stage):
        z_copy(way, c, to, stage, OTHER).wait_recv()

    def yf_copy(c, part):
        return pltpu.make_async_remote_copy(
            src_ref=yfs.at[c, cuts[part], :], dst_ref=yfr.at[c, cuts[part], :],
            send_sem=yf_s.at[part, c], recv_sem=yf_r.at[part, c],
            device_id=target(ACROSS), device_id_type=MESH,
        )

    def x_copy(c, stage):
        return pltpu.make_async_remote_copy(
            src_ref=xs.at[c, spans[stage], :], dst_ref=xr.at[c, spans[stage], :],
            send_sem=x_s.at[stage, c], recv_sem=x_r.at[stage, c],
            device_id={"rep": other}, device_id_type=MESH,
        )

    def contribute(c, m):
        to = nearest(nz - 1 - m)

        @pl.when(c == 0)
        def _():
            cot_cross(to).wait_recv()
            for k in range(1, n_tp):
                cot_share(k, tp, to).start()

        @pl.when(m == 0)
        def _():
            he_cross(c).wait_recv()

        @pl.when(c == 0)
        def _():
            for k in range(1, n_tp):
                cot_share(k, lax.rem(tp + n_tp - k, n_tp), to).wait_recv()

        def term(line):
            return lax.dot_general(
                cot_block(0, 2 * tokens, 2 * to + line), he[:, columns(c)],
                (((0,), (0,)), ((), ())), preferred_element_type=F32,
            )

        value = term(1 - y)
        ys[c, to] = value[:head].astype(BF16)
        y_copy(c, to).start()
        opp[c, to] = value[head:]
        own[c, to] = term(y)


    def forward(s):
        for way, place in ((RIGHT, z), (LEFT, nz - 1 - z)):
            at = s + jnp.where(place == 0, LEAD, 0)
            safe = jnp.maximum(at, 0)
            c = lax.div(safe, nz - 1)
            j = lax.rem(safe, nz - 1) - place

            @pl.when((at >= 0) & (at < chunks * (nz - 1)) & (j >= 0))
            def _():
                to = nz - 1 - j if way == RIGHT else j

                @pl.when(place == 0)
                def _():
                    zs[c, to, mine, :] = own[c, to, second, :].astype(BF16)
                    zs[c, to, cross, :] = opp[c, to].astype(BF16)

                @pl.when(place > 0)
                def _():
                    z_arrived(way, c, to, 0)
                    before = zr.at[way, c, to]
                    zs[c, to, mine, :] = (own[c, to, second, :] + before[mine, :].astype(F32)).astype(BF16)
                    zs[c, to, cross, :] = (opp[c, to] + before[cross, :].astype(F32)).astype(BF16)

                z_copy(way, c, to, 0).start()

    def forward_rest(s):
        for way, place in ((RIGHT, z), (LEFT, nz - 1 - z)):
            at = s + jnp.where(place == 0, LEAD, 0)
            safe = jnp.maximum(at, 0)
            c = lax.div(safe, nz - 1)
            j = lax.rem(safe, nz - 1) - place

            @pl.when((at >= 0) & (at < chunks * (nz - 1)) & (j >= 0))
            def _():
                to = nz - 1 - j if way == RIGHT else j
                y_copy(c, to).wait_recv()

                @pl.when(place == 0)
                def _():
                    zs[c, to, rest, :] = (own[c, to, first, :] + yr[c, to].astype(F32)).astype(BF16)

                @pl.when(place > 0)
                def _():
                    z_arrived(way, c, to, 1)
                    zs[c, to, rest, :] = (
                        own[c, to, first, :] + yr[c, to].astype(F32) + zr[way, c, to, rest, :].astype(F32)
                    ).astype(BF16)

                z_copy(way, c, to, 1).start()

    sides = ((RIGHT, z > 0), (LEFT, z < nz - 1))

    def finish_line(c):
        for way, there in sides:

            @pl.when(there)
            def _():
                z_arrived(way, c, z, 0)
                before = zr.at[way, c, z]
                opp[c, z] += before[cross, :].astype(F32)
                own[c, z, second, :] += before[mine, :].astype(F32)

        yfs[c] = opp[c, z].astype(BF16)
        for part in range(2):
            yf_copy(c, part).start()
        y_copy(c, z).wait_recv()
        own[c, z, first, :] += yr[c, z].astype(F32)
        for way, there in sides:

            @pl.when(there)
            def _():
                z_arrived(way, c, z, 1)
                own[c, z, first, :] += zr[way, c, z, rest, :].astype(F32)

        xs[c, first, :] = own[c, z, first, :].astype(BF16)
        x_copy(c, 0).start()

    def finish_pair(c):
        for part in range(2):
            yf_copy(c, part).wait_recv()
            span = spans[1 + part]
            own[c, z, span, :] += yfr[c, cuts[part], :].astype(F32)
            xs[c, span, :] = own[c, z, span, :].astype(BF16)
            x_copy(c, 1 + part).start()
        lanes = pl.ds(pl.multiple_of(rep * hq + c * width, 128), width)
        gout[:, lanes] = gin[:, lanes] + own[c, z] * scale

    def finish_cross(c):
        lanes = pl.ds(pl.multiple_of(other * hq + c * width, 128), width)
        for stage, span in enumerate(spans):
            x_copy(c, stage).wait_recv()
            gout[span, lanes] = gin[span, lanes] + xr[c, span, :].astype(F32) * scale

    def reduce_step(s):
        def when_due(offset, ready, act):
            at = s - offset
            safe = jnp.maximum(at, 0)
            c = lax.div(safe, nz - 1) + ready

            @pl.when((at >= 0) & (lax.rem(safe, nz - 1) == 0) & (c >= 0) & (c < chunks))
            def _():
                act(c)

        base = s + lead + ahead

        @pl.loop(0, 2)
        def _(turn):
            late_turn = 1 - turn
            c = lax.div(base, nz - 1) - late_turn
            m = lax.rem(base, nz - 1) + late_turn * (nz - 1)

            @pl.when((m < nz) & (c >= 0) & (c < chunks))
            def _():
                contribute(c, m)

        forward(s)
        forward_rest(s - split)
        when_due(settle, -1, finish_line)
        when_due(pair_due, -1, finish_pair)
        when_due(cross_due, -1, finish_cross)

    gather_ticks = 4 * (nz - 1)
    use_ticks = max(2 * n - 3, n + max(USE_LAG))
    last_step = chunks * (nz - 1) + cross_due
    sum_ticks = max(
        START[i] + chunks * (nz - 1) + LEAD + AHEAD[i] + SETTLE[i] + FP[i] + FC[i] for i in range(2)
    )

    def used(k):
        return jnp.clip(jnp.minimum(lax.div(k + 2, 2), k - use_lag) + 1, 1, n)

    def reduce_tick(k):
        step = k - begin - lead - ahead

        @pl.when((k >= begin) & (step < last_step))
        def _():
            reduce_step(step)

    def when_gathering(k, act, *more):
        @pl.when((k >= 0) & (k < gather_ticks) & functools.reduce(jnp.logical_and, more, True))
        def _():
            act(k)

    def tick(k, carry):
        if RSFIRST == 1:
            reduce_tick(k)
        when_gathering(k, gather)
        behind = k - lag
        when_gathering(behind, gather_across, lax.rem(jnp.maximum(behind, 0), 4) == 0)

        @pl.when(k == 1)
        def _():
            piece_arrived(beyond, 0)
            piece(OTHER, beyond, 0).start()

        @pl.when(k == max(START))
        def _():
            loads(6).wait()

        if RSFIRST == 0:
            reduce_tick(k)
        if Y0 > 0:
            at = k - Y0
            when_gathering(at, lambda j: across(j, 0), lax.rem(jnp.maximum(at, 0), 4) == 0)
        at = k - Y1
        when_gathering(at, lambda j: across(j, 1), lax.rem(jnp.maximum(at, 0), 4) == 1, (at < 4) | (Y1H == 0))
        if Y1H:
            when_gathering(k, lambda j: across(j, 1), lax.rem(k, 4) == 1, k >= 4)
        if HOLD:
            when_gathering(k - HOLD, held)
        if YI >= 0:

            @pl.when(k == YI)
            def _():
                piece(ACROSS, me, 1).start()

        if RSFIRST == 2:
            reduce_tick(k)
        lax.fori_loop(jnp.where(k == 0, 0, used(k - 1)), used(k), use, 0)
        return carry

    lax.fori_loop(0, max(use_ticks, gather_ticks, sum_ticks), tick, 0)

    @pl.loop(0, tokens // TILE)
    def _(i):
        span = tile_at(i)
        gate = ge[span, :].astype(F32)
        sig = 1.0 / (1.0 + jnp.exp(-gate))
        grad = hg[span, :]
        ug[span, :] = (grad * (gate * sig)).astype(BF16)
        gg[span, :] = (
            grad * ue[span, :].astype(F32) * sig * (1.0 + gate * (1.0 - sig))
        ).astype(BF16)

    @pl.loop(0, n)
    def _(shard):
        for k in range(1, n_tp):
            share_arrived(k, shard)
        total = part[0, shard].astype(F32)
        for j in range(1, n_tp):
            total = total + part[j, shard].astype(F32)
        if flat:
            late[:, pl.ds(pl.multiple_of(shard * rows, rows), rows)] = total.astype(BF16)
        else:
            late[shard] = total.astype(BF16)

    reduce_step(jnp.int32(last_step))

    for p in range(3):
        piece(ACROSS, me, p).wait_send()

    @pl.loop(0, nz)
    def _(at):
        same = 2 * at + y
        crossed = 2 * at + 1 - y

        @pl.when((at <= z) & (z < nz - 1))
        def _():
            for p in range(3):
                piece(RIGHT, same, p).wait_send()
            piece(RIGHT, crossed, 2).wait_send()

        @pl.when((at >= z) & (z > 0))
        def _():
            for p in range(3):
                piece(LEFT, same, p).wait_send()
            piece(LEFT, crossed, 2).wait_send()

        piece(OTHER, crossed, 0).wait_send()
        cot_cross(at).wait_send()

        @pl.when(at != z)
        def _():
            piece(OTHER, same, 0).wait_send()
            for p in range(2):
                piece(ACROSS, same, p).wait_send()

        for k in range(1, n_tp):
            cot_share(k, tp, at).wait_send()
            share(k, same).wait_send()
            share(k, crossed).wait_send()

        @pl.loop(0, chunks)
        def _(c):
            y_copy(c, at).wait_send()

            @pl.when(at > z)
            def _():
                z_copy(RIGHT, c, at, 0).wait_send()
                z_copy(RIGHT, c, at, 1).wait_send()

            @pl.when(at < z)
            def _():
                z_copy(LEFT, c, at, 0).wait_send()
                z_copy(LEFT, c, at, 1).wait_send()

    @pl.loop(0, chunks)
    def _(c):
        he_cross(c).wait_send()
        for part in range(2):
            yf_copy(c, part).wait_send()
        for stage in range(3):
            x_copy(c, stage).wait_send()


def deliver(*refs):
    count = 4
    sems = refs[-1]
    copies = [
        pltpu.make_async_copy(refs[i], refs[count + i], sems.at[i]) for i in range(count)
    ]
    for copy in copies:
        copy.start()
    for copy in copies:
        copy.wait()


def solution(mesh):
    n, n_tp, n_rep = mesh.shape["fs"], mesh.shape["tp"], mesh.shape["rep"]
    assert n_rep == 2 and n % 2 == 0 and n >= 8

    def per_device(gl, ul, ge, ue, cotangent, w, gin):
        tokens, cols = gl.shape
        rows, width = w.shape[0], cotangent.shape[1]
        assert rows % 64 == 0 and cols % 256 == 0
        nz, hq = n // 2, cols // 2
        head = max(rows * H0 // 256, 1) * 16
        tail = rows - head
        chunks = min(CHUNKS, hq // 128)
        scale = 1.0 / math.sqrt(tokens * n_rep * n)
        whole_lanes = rows % 128 == 0
        cot = cotangent
        if not whole_lanes:
            cot = cotangent.reshape(tokens, n, rows).transpose(1, 0, 2)
        cot_both = (2 * tokens, width) if whole_lanes else (n, 2 * tokens, rows)
        vmem = pl.BlockSpec(memory_space=pltpu.VMEM)
        dma = pltpu.SemaphoreType.DMA
        part = hq // chunks
        late, gg, ug, gout = pl.pallas_call(
            functools.partial(kernel, n, n_tp, chunks, scale),
            out_shape=(
                pltpu.VMEM(cot.shape, BF16),
                pltpu.VMEM((tokens, cols), BF16),
                pltpu.VMEM((tokens, cols), BF16),
                pltpu.VMEM((rows, cols), F32),
            ),
            in_specs=[pl.BlockSpec(memory_space=pl.ANY)] * 7,
            out_specs=(vmem,) * 4,
            scratch_shapes=[
                pltpu.VMEM((tokens, cols), BF16),
                pltpu.VMEM((tokens, cols), BF16),
                pltpu.VMEM((tokens, cols), BF16),
                pltpu.VMEM((tokens, cols), BF16),
                pltpu.VMEM(cot_both, BF16),
                pltpu.VMEM((rows, cols), F32),
                pltpu.VMEM((n, rows, cols), BF16),
                pltpu.VMEM((tokens, cols), BF16),
                pltpu.VMEM((2 * tokens, hq), BF16),
                pltpu.VMEM((tokens, hq), BF16),
                pltpu.VMEM((tokens, cols), F32),
                pltpu.VMEM((n_tp, n, tokens, rows), BF16),
                pltpu.VMEM((chunks, nz, rows, part), F32),
                pltpu.VMEM((chunks, nz, tail, part), F32),
                pltpu.VMEM((chunks, nz, head, part), BF16),
                pltpu.VMEM((chunks, nz, head, part), BF16),
                pltpu.VMEM((chunks, nz, rows + tail, part), BF16),
                pltpu.VMEM((2, chunks, nz, rows + tail, part), BF16),
                pltpu.VMEM((chunks, tail, part), BF16),
                pltpu.VMEM((chunks, tail, part), BF16),
                pltpu.VMEM((chunks, rows, part), BF16),
                pltpu.VMEM((chunks, rows, part), BF16),
                dma((7,)),
                dma((4, n, 3)),
                dma((n, 4)),
                dma((nz,)),
                dma((nz,)),
                dma((n_tp, nz)),
                dma((n_tp, nz)),
                dma((chunks,)),
                dma((chunks,)),
                dma((chunks, nz)),
                dma((chunks, nz)),
                dma((2, chunks, nz)),
                dma((4, chunks, nz)),
                dma((2, chunks)),
                dma((2, chunks)),
                dma((3, chunks)),
                dma((3, chunks)),
                dma((n_tp, n)),
                dma((n_tp, n)),
            ],
            compiler_params=pltpu.CompilerParams(
                collective_id=0, has_side_effects=True, vmem_limit_bytes=LIMIT
            ),
        )(gl, ul, ge, ue, cot, w, gin)
        late, gg, ug, gout = pl.pallas_call(
            deliver,
            out_shape=tuple(jax.ShapeDtypeStruct(a.shape, a.dtype) for a in (late, gg, ug, gout)),
            in_specs=[pl.BlockSpec(memory_space=pl.ANY)] * 4,
            out_specs=(pl.BlockSpec(memory_space=pl.ANY),) * 4,
            scratch_shapes=[dma((4,))],
            compiler_params=pltpu.CompilerParams(vmem_limit_bytes=1 << 20),
        )(late, gg, ug, gout)
        if not whole_lanes:
            late = late.transpose(1, 0, 2).reshape(tokens, width)
        return late, gg, ug, gout

    placed = (
        P(("rep", "fs"), "tp"),
        P(("rep", "fs"), "tp"),
        P(("rep", "fs"), "tp"),
        P(("rep", "fs"), "tp"),
        P(("rep", "fs"), None),
        P("fs", "tp"),
        P("fs", "tp"),
    )
    return jax.shard_map(
        per_device,
        mesh=mesh,
        in_specs=placed,
        out_specs=(
            P(("rep", "fs"), None),
            P(("rep", "fs"), "tp"),
            P(("rep", "fs"), "tp"),
            P("fs", "tp"),
        ),
        check_vma=False,
    )
```
